512 devices in a mesh: kv: 64 (over z, y), tp: 8 (over x, core).
Axes of the slice: x: 4, y: 4, z: 16, core: 2. Of those that a mesh axis runs over, the one named last changes fastest.
Arguments:
- queries: bfloat16 [16384, 1024], P('kv', 'tp'), may hold values from -4 to 4
- keys: bfloat16 [16384, 1024], P('kv', 'tp'), may hold values from -4 to 4
- values: bfloat16 [16384, 1024], P('kv', 'tp'), may hold values from -5 to 5
- log_sums: float32 [16, 16384], P('tp', 'kv'), may hold values from 5.5 to 7
- out_grad: bfloat16 [16384, 1024], P('kv', 'tp'), may hold values from -24 to 24
- chosen: int32 [128, 8], P('kv'), may hold values from -1 to 511, as said below
- normed: bfloat16 [16384, 2048], P('kv', 'tp'), may hold values from -0.23925781 to 0.23925781
Outputs:
- query_grad: bfloat16 [16384, 1024], P('kv', 'tp')
- key_grad: bfloat16 [16384, 1024], P('kv', 'tp')
- value_grad: bfloat16 [16384, 1024], P('kv', 'tp')
- weight_grad: float32 [2048, 1024], P('kv', 'tp')
The draws below stay inside these ranges and needn't reach their ends.
Inputs may be any that keep to these rules, and one draw needn't show every extreme that they name: `chosen`: each used entry names a key block that ends at or before its query block's start; the used entries of one list are distinct. Among the lists of the 2 query blocks of one index of kv, the key blocks of any other index of kv appear as at most one distinct block; for every index from 1 on, the first query block's list names a block of the index before, and the last index's first query block's list names a block of index 0. Blocks of the own index of kv before the query block may appear freely.
All inputs are finite; a program needn't handle non-finite values.
Results may differ from the reference program's by a relative error of at most 0.008.
Values may be sent and summed in bfloat16 or wider, within the bound.
No kernel may reach another device: no remote copies, remote signals or barrier semaphores. Data moves between devices by JAX's collectives and lax.ppermute only.
A program may use at most 64 MiB of HBM per device.

```python
import jax
import jax.numpy as jnp
from jax import lax

D = 2048
HEADS = 16
HD = 64
QB = 128
KB = 32
SEL = 8
TOKENS = 16384
QBLK_DEV = 2
KBLK_DEV = 8
NQB = 128
KEY_BLOCK_TOTAL = 512


def draw_chosen(key, part):
    device_count = KEY_BLOCK_TOTAL // KBLK_DEV
    first_key, second_key, third_key, fourth_key = jax.random.split(key, 4)
    favoured = jax.random.randint(first_key, (device_count,), 0, KBLK_DEV, dtype=jnp.int32)
    spread_pick = jax.random.randint(second_key, (device_count, device_count), 0, KBLK_DEV, dtype=jnp.int32)
    coin_toss = jax.random.randint(third_key, (device_count, device_count), 0, 4, dtype=jnp.int32)
    pool_offset = jnp.where(coin_toss < 3, favoured[None, :], spread_pick)
    block_numbers = jnp.arange(KEY_BLOCK_TOTAL, dtype=jnp.int32)
    query_ids = jnp.arange(NQB, dtype=jnp.int32)
    holder = (query_ids // QBLK_DEV)[:, None]
    inner = (query_ids % QBLK_DEV)[:, None]
    owner_ids = (block_numbers // KBLK_DEV)[None, :]
    offset_ids = (block_numbers % KBLK_DEV)[None, :]
    pool_pick = pool_offset[holder, owner_ids]
    from_pool = (owner_ids < holder) & (offset_ids == pool_pick)
    from_own = (owner_ids == holder) & (offset_ids < inner * (QB // KB))
    eligible_blocks = from_pool | from_own
    rank_order = jax.random.randint(fourth_key, (NQB, KEY_BLOCK_TOTAL), 0, 4096, dtype=jnp.int32)
    preceding_single = (owner_ids == holder - 1) & (inner == 0)
    halfway_distance = (owner_ids == holder - device_count // 2) & (inner == min(1, QBLK_DEV - 1))
    farthest_pair = (owner_ids == 0) & (holder == device_count - 1) & (inner == 0)
    extra_reward = jnp.where(preceding_single | halfway_distance | farthest_pair, 8192, 0).astype(jnp.int32)
    graded_blocks = jnp.where(eligible_blocks, (rank_order + extra_reward) * KEY_BLOCK_TOTAL + block_numbers[None, :], -1).astype(jnp.int32)
    top_scores, top_ids = lax.top_k(graded_blocks, SEL)
    return jnp.where(top_scores >= 0, top_ids, -1).astype(jnp.int32)


def with_spikes(drawn, rng, source, target, shards_of, factor):
    owner, partner = [(jnp.arange(drawn.shape[axis_at]) // (drawn.shape[axis_at] // shards_of)).reshape([-1 if axis == axis_at else 1 for axis in range(drawn.ndim)]) for axis_at in (source, target)]
    chosen = jax.random.permutation(rng, shards_of)[partner]
    strong = (owner == chosen) | (owner == (partner + shards_of // 2) % shards_of)
    return jnp.where(strong, factor * drawn, drawn)


def block_scale(own_key, dims, shards, least, high):
    gain, own = 1.0, jax.random.fold_in(own_key, 6)
    for dim, blocks in shards:
        steps = jnp.exp(jax.random.uniform(jax.random.fold_in(own, dim), (blocks,), jnp.float32, least / len(shards), high / len(shards)))
        gain = gain * jnp.repeat(steps, dims[dim] // blocks).reshape([-1 if axis == dim else 1 for axis in range(len(dims))])
    return gain


def gaussian(own_key, shape, deviation, limit, cuts=(), kind=jnp.bfloat16):
    result = deviation * jax.random.normal(own_key, shape, jnp.float32)
    if cuts:
        result = result * block_scale(own_key, shape, cuts, -0.22, 0.18)
    return jnp.clip(result, -limit, limit).astype(kind)


def heavy_noise(stream_key, shape, scale, bound, cuts, heavy, held_as=jnp.bfloat16):
    values = scale * jax.random.normal(stream_key, shape, jnp.float32)
    if cuts:
        values = values * block_scale(stream_key, shape, cuts, -0.22, 0.18)
    return jnp.clip(with_spikes(values, jax.random.fold_in(stream_key, 3), *heavy), -bound, bound).astype(held_as)


def setup_inputs(seed: int = 0) -> dict:
    splits = jax.random.split(jax.random.key(seed), 8)
    queries = gaussian(splits[0], (TOKENS, HEADS * HD), 1.0, 4.0, ((0, 64), (1, 8)))
    keys = gaussian(splits[1], (TOKENS, HEADS * HD), 1.0, 4.0, ((0, 64), (1, 8)))
    values = gaussian(splits[2], (TOKENS, HEADS * HD), 1.0, 5.0, ((0, 64), (1, 8)))
    log_sums = jnp.clip(5.5 + 1.5 * jax.random.uniform(splits[3], (HEADS, TOKENS), jnp.float32) ** block_scale(splits[3], (HEADS, TOKENS), ((0, 8), (1, 64)), -0.2, 0.2), 5.5, 7.0)
    out_grad = gaussian(splits[4], (TOKENS, HEADS * HD), 4.0, 24.0, ((0, 64), (1, 8)))
    chosen = draw_chosen(jax.random.fold_in(splits[7], 71), 0)
    normed = heavy_noise(splits[6], (TOKENS, D), 0.03, 0.23925781, ((0, 64), (1, 8)), (0, 1, 64, 4.0))
    return {"queries": queries, "keys": keys, "values": values, "log_sums": log_sums, "out_grad": out_grad, "chosen": chosen, "normed": normed}


def rounded(array):
    return lax.optimization_barrier(array.astype(jnp.bfloat16)).astype(jnp.float32)


def block_grads(inputs, scaling):
    query_blk, grad_blk, sums_blk, keys_sel, vals_sel, keys_own, vals_own, eligible_blocks = inputs
    span_rows = query_blk.shape[0]
    scores = jnp.einsum("qhd,skhd->hqsk", query_blk, keys_sel) * scaling
    weights = jnp.where(eligible_blocks[None, None, :, None], jnp.exp(scores - sums_blk[:, :, None, None]), 0.0)
    causal = lax.broadcasted_iota(jnp.int32, (span_rows, span_rows), 0) >= lax.broadcasted_iota(jnp.int32, (span_rows, span_rows), 1)
    own_scores = jnp.einsum("qhd,khd->hqk", query_blk, keys_own) * scaling
    own_weights = jnp.where(causal[None], jnp.exp(own_scores - sums_blk[:, :, None]), 0.0)
    weights_low = rounded(weights)
    own_low = rounded(own_weights)
    attended = jnp.einsum("hqsk,skhd->qhd", weights_low, vals_sel) + jnp.einsum("hqk,khd->qhd", own_low, vals_own)
    deltas = jnp.sum(grad_blk * attended, axis=-1).T
    dots_sel = jnp.einsum("qhd,skhd->hqsk", grad_blk, vals_sel)
    own_dots = jnp.einsum("qhd,khd->hqk", grad_blk, vals_own)
    slopes = rounded(weights * (dots_sel - deltas[:, :, None, None]))
    own_slopes = rounded(own_weights * (own_dots - deltas[:, :, None]))
    query_part = scaling * (jnp.einsum("hqsk,skhd->qhd", slopes, keys_sel) + jnp.einsum("hqk,khd->qhd", own_slopes, keys_own))
    key_terms = scaling * jnp.einsum("hqsk,qhd->skhd", slopes, query_blk)
    value_terms = jnp.einsum("hqsk,qhd->skhd", weights_low, grad_blk)
    own_key_terms = scaling * jnp.einsum("hqk,qhd->khd", own_slopes, query_blk)
    own_value_terms = jnp.einsum("hqk,qhd->khd", own_low, grad_blk)
    return query_part.astype(jnp.bfloat16), key_terms, value_terms, own_key_terms, own_value_terms


def reference(queries, keys, values, log_sums, out_grad, chosen, normed):
    rows_all, columns = queries.shape
    head_count = log_sums.shape[0]
    head_size = columns // head_count
    query_blocks = rows_all // QB
    key_blocks = rows_all // KB
    selected = chosen.shape[1]
    scaling = head_size ** -0.5
    eligible_blocks = chosen >= 0
    picked = jnp.clip(chosen, 0, key_blocks - 1).astype(jnp.int32)
    query_full = queries.astype(jnp.float32).reshape(rows_all, head_count, head_size)
    key_full = keys.astype(jnp.float32).reshape(rows_all, head_count, head_size)
    value_full = values.astype(jnp.float32).reshape(rows_all, head_count, head_size)
    grad_full = out_grad.astype(jnp.float32).reshape(rows_all, head_count, head_size)
    offsets_kb = jnp.arange(KB, dtype=jnp.int32)

    def step(carry, index):
        key_acc, value_acc = carry
        first_row = (index * QB).astype(jnp.int32)
        query_blk = lax.dynamic_slice_in_dim(query_full, first_row, QB, 0)
        grad_blk = lax.dynamic_slice_in_dim(grad_full, first_row, QB, 0)
        sums_blk = lax.dynamic_slice_in_dim(log_sums, first_row, QB, 1)
        rows_sel = (picked[index][:, None] * KB + offsets_kb[None, :]).reshape(-1)
        keys_sel = key_full[rows_sel].reshape(selected, KB, head_count, head_size)
        vals_sel = value_full[rows_sel].reshape(selected, KB, head_count, head_size)
        keys_own = lax.dynamic_slice_in_dim(key_full, first_row, QB, 0)
        vals_own = lax.dynamic_slice_in_dim(value_full, first_row, QB, 0)
        query_part, key_terms, value_terms, own_key_terms, own_value_terms = block_grads(
            (query_blk, grad_blk, sums_blk, keys_sel, vals_sel, keys_own, vals_own, eligible_blocks[index]), scaling)
        key_acc = key_acc.at[rows_sel].add(key_terms.reshape(-1, head_count, head_size))
        value_acc = value_acc.at[rows_sel].add(value_terms.reshape(-1, head_count, head_size))
        key_acc = lax.dynamic_update_slice_in_dim(key_acc, lax.dynamic_slice_in_dim(key_acc, first_row, QB, 0) + own_key_terms, first_row, 0)
        value_acc = lax.dynamic_update_slice_in_dim(value_acc, lax.dynamic_slice_in_dim(value_acc, first_row, QB, 0) + own_value_terms, first_row, 0)
        return (key_acc, value_acc), query_part

    zeros_acc = jnp.zeros((rows_all, head_count, head_size), jnp.float32)
    (key_acc, value_acc), query_parts = lax.scan(step, (zeros_acc, zeros_acc), jnp.arange(query_blocks, dtype=jnp.int32))
    query_grad = query_parts.reshape(rows_all, columns)
    key_grad = key_acc.reshape(rows_all, columns).astype(jnp.bfloat16)
    value_grad = value_acc.reshape(rows_all, columns).astype(jnp.bfloat16)
    weight_grad = jnp.dot(normed.T, value_grad, preferred_element_type=jnp.float32)
    return query_grad, key_grad, value_grad, weight_grad
```

```python
import jax
import jax.numpy as jnp
from jax import lax
from jax.experimental import pallas as pl
from jax.experimental.pallas import tpu as pltpu
from jax.sharding import Mesh
from jax.sharding import PartitionSpec as P

KV = ("z", "y")
TP = ("x", "c")
QB = 128
KB = 32
HD = 64
SEL = 8
F32 = jnp.float32
BF16 = jnp.bfloat16


def iota(shape, dim):
    return lax.broadcasted_iota(jnp.int32, shape, dim)


def swap(x):
    return pltpu.roll(x, HD, 1)


def side_by_side(a, b):
    low = iota(a.shape, 1) < HD
    return jnp.where(low, a, swap(b)), jnp.where(low, swap(a), b)


def dot(a, b, dims=((1,), (0,))):
    return lax.dot_general(a, b, (dims, ((), ())), preferred_element_type=F32)


def pack_kernel(base_ref, chosen_ref, keys_ref, values_ref, out_ref):
    rows = keys_ref.shape[0]
    blocks = rows // KB
    packs = side_by_side(keys_ref[...].astype(F32), values_ref[...].astype(F32))
    lane = iota((1, 128), 1)
    high = jnp.zeros((1, 128), F32)
    low = jnp.zeros((1, 128), F32)
    for g in range(2):
        for s in range(SEL):
            entry = chosen_ref[g, s] + 1
            here = lane == base_ref[0] + (g * SEL + s)
            high = jnp.where(here, (entry >> 3).astype(F32), high)
            low = jnp.where(here, (entry & 7).astype(F32), low)
    shape = (KB * 16, rows)
    row, col = iota(shape, 0), iota(shape, 1)
    kind = row & 15
    perm = jnp.where((kind < blocks) & (col == kind * KB + (row >> 4)), 1.0, 0.0).astype(BF16)
    kind = iota((KB * 16, 128), 0) & 15
    extra = jnp.where(kind == 8, high, 0.0) + jnp.where(kind == 9, low, 0.0)
    for h in range(2):
        out_ref[h * KB * 16 : (h + 1) * KB * 16, :] = (dot(perm, packs[h].astype(BF16)) + extra).astype(BF16)


def select_kernel(got_ref, out_ref, ids_ref):
    got = got_ref[...].astype(F32).reshape(64, 2, 8, 128)
    table = got[:, 0].reshape(512, 128).astype(BF16)
    meta = got[:, 1].reshape(8, 8, 8, 128).sum(axis=1)
    ids = meta[:, 0] * 8.0 + meta[:, 1]
    ids_ref[...] = ids
    columns = ids.T
    number = (iota((128, 512), 1) + 1).astype(F32)
    for j in range(8):
        hot = jnp.where(number == columns[:, j : j + 1], 1.0, 0.0).astype(BF16)
        out_ref[j * 128 : (j + 1) * 128, :] = dot(hot, table).astype(BF16)


def attend_kernel(chosen_ref, queries_ref, keys_ref, values_ref, grad_ref, sums_ref, got_ref, dq_ref, back_ref, own_ref):
    lane = iota((QB, 128), 1)
    causal = iota((QB, QB), 0) <= iota((QB, QB), 1)
    sub = iota((SEL, QB), 0)
    for g in range(2):
        span = slice(g * QB, (g + 1) * QB)
        own_packs = side_by_side(keys_ref[span, :].astype(F32), values_ref[span, :].astype(F32))
        q = queries_ref[span, :].astype(F32) * (HD**-0.5)
        do = grad_ref[span, :].astype(F32)
        used = jnp.zeros((SEL, QB), jnp.int32)
        for s in range(SEL):
            used = jnp.where(sub == s, chosen_ref[g, s] + 1, used)
        used = (used > 0)[None]
        dq_parts = []
        for h in range(2):
            chosen_rows = got_ref[h * KB : (h + 1) * KB].astype(F32)[:, g * SEL : (g + 1) * SEL, :]
            pairs = jnp.concatenate([chosen_rows.reshape(KB * SEL, 128), own_packs[h]], axis=0).astype(BF16)
            q_low = jnp.where(lane < HD, q if h == 0 else swap(q), 0.0).astype(BF16)
            do_high = jnp.where(lane >= HD, do if h == 1 else swap(do), 0.0).astype(BF16)
            scores = dot(pairs, q_low, ((1,), (1,)))
            dots = dot(pairs, do_high, ((1,), (1,)))
            raw = jnp.exp(scores - sums_ref[h : h + 1, span])
            picked = jnp.where(used, raw[: KB * SEL].reshape(KB, SEL, QB), 0.0).reshape(KB * SEL, QB)
            weights = jnp.concatenate([picked, jnp.where(causal, raw[KB * SEL :], 0.0)], axis=0)
            low = weights.astype(BF16)
            deltas = jnp.sum(low.astype(F32) * dots, axis=0, keepdims=True)
            slopes = (weights * (dots - deltas)).astype(BF16)
            terms = dot(slopes, q_low) + dot(low, do_high)
            back_ref[h * KB : (h + 1) * KB, g * SEL : (g + 1) * SEL, :] = (
                terms[: KB * SEL].reshape(KB, SEL, 128).astype(BF16)
            )
            own_ref[h, span, :] = terms[KB * SEL :]
            dq_parts.append(dot(slopes, pairs, ((0,), (0,))) * (HD**-0.5))
        dq_ref[span, :] = jnp.where(lane < HD, dq_parts[0], swap(dq_parts[1])).astype(BF16)


def gather_kernel(ids_ref, got_ref, out_ref):
    number = (iota((512, 128), 0) + 1).astype(F32)
    total = jnp.zeros((512, 128), F32)
    for j in range(8):
        hot = jnp.where(number == ids_ref[j : j + 1, :], 1.0, 0.0).astype(BF16)
        total = total + dot(hot, got_ref[j * 128 : (j + 1) * 128, :])
    out_ref[...] = total.astype(BF16)


def finish_kernel(got_ref, own_ref, normed_ref, dk_ref, dv_ref, part_ref):
    rows = own_ref.shape[1]
    row, col = iota((rows, rows), 0), iota((rows, rows), 1)
    perm = jnp.where(col == (row & (KB - 1)) * 8 + (row >> 5), 1.0, 0.0).astype(BF16)
    first = dot(perm, got_ref[:rows, :]) + own_ref[0]
    second = dot(perm, got_ref[rows:, :]) + own_ref[1]
    low = iota((rows, 128), 1) < HD
    dk_ref[...] = jnp.where(low, first, swap(second)).astype(BF16)
    dv = jnp.where(low, swap(first), second).astype(BF16)
    dv_ref[...] = dv
    for t in range(8):
        part = dot(normed_ref[t], dv).astype(BF16)
        for zz in range(2):
            for y in range(4):
                k = zz * 4 + y
                part_ref[y, t * 2 + zz] = part[k * 32 : (k + 1) * 32, :]


VM = pl.BlockSpec(memory_space=pltpu.VMEM)
SM = pl.BlockSpec(memory_space=pltpu.SMEM)


def call(kernel, out, specs, name, *args):
    return pl.pallas_call(
        kernel,
        out_shape=out,
        in_specs=specs,
        out_specs=jax.tree.map(lambda _: VM, out),
        name=name,
    )(*args)


def shape(*dims, dtype=BF16):
    return jax.ShapeDtypeStruct(dims, dtype)


def exchange(x, axis):
    return lax.all_to_all(x, axis, split_axis=0, concat_axis=0, tiled=True)


def body(queries, keys, values, log_sums, out_grad, chosen, normed):
    rows = queries.shape[0]
    base = ((lax.axis_index(KV) % 8) * 16).astype(jnp.int32).reshape(1)
    with jax.named_scope("pieces"):
        pieces = call(pack_kernel, shape(1024, 128), [SM, SM, VM, VM], "pack", base, chosen, keys, values)
        pieces = exchange(pieces.reshape(64, 16, 128), KV)
    with jax.named_scope("features"):
        features = exchange(jnp.broadcast_to(normed.T[None], (8, *normed.shape)), TP)
    with jax.named_scope("picked"):
        picked, ids = call(
            select_kernel, (shape(1024, 128), shape(8, 128, dtype=F32)), [VM], "select", pieces.reshape(1024, 128)
        )
        picked = exchange(picked.reshape(64, 16, 128), KV)
    with jax.named_scope("attend"):
        query_grad, back, own = call(
            attend_kernel,
            (shape(rows, 128), shape(64, 16, 128), shape(2, rows, 128, dtype=F32)),
            [SM] + [VM] * 6,
            "attend",
            chosen, queries, keys, values, out_grad, log_sums, picked,
        )
    with jax.named_scope("back"):
        back = exchange(back, KV)
    with jax.named_scope("owner"):
        totals = call(gather_kernel, shape(512, 128), [VM, VM], "gather", ids, back.reshape(1024, 128))
        totals = exchange(totals.reshape(64, 8, 128), KV)
    with jax.named_scope("finish"):
        key_grad, value_grad, part = call(
            finish_kernel,
            (shape(rows, 128), shape(rows, 128), shape(4, 16, 32, 128)),
            [VM] * 3,
            "finish",
            totals.reshape(512, 128), own, features,
        )
    with jax.named_scope("sum_y"):
        part = exchange(part, "y").astype(F32).sum(axis=0).astype(BF16)
    with jax.named_scope("sum_z"):
        weight_grad = exchange(part, "z").astype(F32).sum(axis=0)
    return query_grad, key_grad, value_grad, weight_grad


def solution(mesh):
    fine = Mesh(mesh.devices.reshape(16, 4, 4, 2), ("z", "y", "x", "c"))
    both = P(KV, TP)
    in_specs = (both, both, both, P(TP, KV), both, P(KV, None), both)
    return jax.shard_map(body, mesh=fine, in_specs=in_specs, out_specs=(both,) * 4, check_vma=False)
```

```python
import jax
import jax.numpy as jnp
from jax import lax
from jax.experimental import pallas as pl
from jax.experimental.pallas import tpu as pltpu
from jax.sharding import Mesh
from jax.sharding import PartitionSpec as P


KV = ("z", "y")
QB = 128
KB = 32
HD = 64
SEL = 8
F32 = jnp.float32
BF16 = jnp.bfloat16


def iota(shape, dim):
    return lax.broadcasted_iota(jnp.int32, shape, dim)


def dot(a, b, dims=((1,), (0,))):
    return lax.dot_general(a, b, (dims, ((), ())), preferred_element_type=F32)


def one_hot(hits):
    return jnp.where(hits, 1.0, 0.0).astype(BF16)


def pack_kernel(base_ref, chosen_ref, keys_ref, values_ref, out_ref):
    lane = iota((1, 128), 1)
    high = jnp.zeros((1, 128), F32)
    low = jnp.zeros((1, 128), F32)
    for g in range(2):
        for s in range(SEL):
            entry = chosen_ref[g, s] + 1
            here = lane == base_ref[0] + (g * SEL + s)
            high = jnp.where(here, (entry >> 3).astype(F32), high)
            low = jnp.where(here, (entry & 7).astype(F32), low)
    row, col = iota((KB * 16, 256), 0), iota((KB * 16, 256), 1)
    kind = row & 15
    perm = one_hot((kind < 8) & (col == kind * KB + (row >> 4)))
    kind = iota((KB * 16, 128), 0) & 15
    extra = jnp.where(kind == 8, high, 0.0) + jnp.where(kind == 9, low, 0.0)
    out_ref[: KB * 16, :] = (dot(perm, keys_ref[...]) + extra).astype(BF16)
    out_ref[KB * 16 :, :] = (dot(perm, values_ref[...]) + extra).astype(BF16)


def select_kernel(got_ref, out_ref, ids_ref):
    got = got_ref[...].astype(F32).reshape(64, 2, 8, 128)
    table = got[:, 0].reshape(512, 128).astype(BF16)
    meta = got[:, 1].reshape(8, 8, 8, 128).sum(axis=1)
    ids = meta[:, 0] * 8.0 + meta[:, 1]
    ids_ref[...] = ids
    columns = ids.T
    number = (iota((128, 512), 1) + 1).astype(F32)
    for j in range(8):
        hot = one_hot(number == columns[:, j : j + 1])
        out_ref[j * 128 : (j + 1) * 128, :] = dot(hot, table).astype(BF16)


def by_rest():
    row, col = iota((256, 256), 0), iota((256, 256), 1)
    return one_hot(col == (row & 7) * KB + ((row >> 3) & 7) * 4 + (row >> 6))


def attend_kernel(
    place_ref, chosen_ref, queries_ref, keys_ref, values_ref, grad_ref, sums_ref, got_ref, dq_ref, back_ref, own_ref
):
    lane = iota((QB, 128), 1)
    causal = iota((QB, QB), 0) <= iota((QB, QB), 1)
    sub = iota((SEL, QB), 0)
    own_k, own_v = [], []
    for g in range(2):
        span = slice(g * QB, (g + 1) * QB)
        got = got_ref[...].astype(F32)[:, g * SEL : (g + 1) * SEL, :].reshape(2, KB * SEL, 128).astype(BF16)
        keys = jnp.concatenate([got[0], keys_ref[span, :]], axis=0)
        values = jnp.concatenate([got[1], values_ref[span, :]], axis=0)
        q = queries_ref[span, :].astype(F32) * (HD**-0.5)
        do = grad_ref[span, :].astype(F32)
        used = jnp.zeros((SEL, QB), jnp.int32)
        for s in range(SEL):
            used = jnp.where(sub == s, chosen_ref[g, s] + 1, used)
        used = (used > 0)[None]
        dq_parts, dk, dv = [], 0.0, 0.0
        for h in range(2):
            mine = (lane >= HD) == (h == 1)
            q_h = jnp.where(mine, q, 0.0).astype(BF16)
            do_h = jnp.where(mine, do, 0.0).astype(BF16)
            scores = dot(keys, q_h, ((1,), (1,)))
            dots = dot(values, do_h, ((1,), (1,)))
            raw = jnp.exp(scores - sums_ref[h : h + 1, span])
            picked = jnp.where(used, raw[: KB * SEL].reshape(KB, SEL, QB), 0.0).reshape(KB * SEL, QB)
            weights = jnp.concatenate([picked, jnp.where(causal, raw[KB * SEL :], 0.0)], axis=0)
            low = weights.astype(BF16)
            deltas = jnp.sum(low.astype(F32) * dots, axis=0, keepdims=True)
            slopes = (weights * (dots - deltas)).astype(BF16)
            dk = dk + dot(slopes, q_h)
            dv = dv + dot(low, do_h)
            dq_parts.append(dot(slopes, keys, ((0,), (0,))))
        back_ref[:KB, g * SEL : (g + 1) * SEL, :] = dk[: KB * SEL].reshape(KB, SEL, 128).astype(BF16)
        back_ref[KB:, g * SEL : (g + 1) * SEL, :] = dv[: KB * SEL].reshape(KB, SEL, 128).astype(BF16)
        own_k.append(dk[KB * SEL :])
        own_v.append(dv[KB * SEL :])
        dq_ref[span, :] = (jnp.where(lane < HD, dq_parts[0], dq_parts[1]) * (HD**-0.5)).astype(BF16)
    perm = by_rest()
    for n, own in enumerate((own_k, own_v)):
        own = dot(perm, jnp.concatenate(own, axis=0).astype(BF16)).astype(BF16)
        for y in range(4):
            own_ref[(y - place_ref[0]) & 3, n] = own[y * 64 : (y + 1) * 64]


def gather_kernel(ids_ref, got_ref, out_ref):
    number = (iota((512, 128), 0) + 1).astype(F32)
    total = jnp.zeros((512, 128), F32)
    for j in range(8):
        hot = one_hot(number == ids_ref[j : j + 1, :])
        total = total + dot(hot, got_ref[j * 128 : (j + 1) * 128, :])
    out_ref[...] = total.astype(BF16)


def add_kernel(place_ref, got_ref, o0_ref, o1_ref, o2_ref, o3_ref, out_ref, acc_ref):
    acc_ref[...] = got_ref[...].astype(F32).reshape(2, 8, 4, 8, 128)
    for s, o_ref in enumerate((o0_ref, o1_ref, o2_ref, o3_ref)):
        y = (place_ref[0] - s) & 3
        acc_ref[:, :, y] = acc_ref[:, :, y] + o_ref[...].astype(F32).reshape(2, 8, 8, 128)
    values = acc_ref[1].reshape(256, 128).astype(BF16)
    for y in range(4):
        out_ref[y, :256, :] = values
        out_ref[y, 256:, :] = acc_ref[0, :, y].reshape(64, 128).astype(BF16)


def turn_kernel(place_ref, normed_ref, out_ref):
    turned = dot(normed_ref[...], by_rest(), ((0,), (1,))).astype(BF16).reshape(2, 4, 32, 256)
    for y in range(4):
        for zz in range(2):
            out_ref[(y - place_ref[0]) & 3, zz * 32 : (zz + 1) * 32, :] = turned[zz, y]


def finish_kernel(place_ref, got_ref, f0_ref, f1_ref, f2_ref, f3_ref, dk_ref, dv_ref, part_ref, acc_ref):
    got = got_ref[...].astype(F32)
    acc_ref[...] = got[:, :256].reshape(4, 8, 4, 8, 128)
    total = 0.0
    for s in range(4):
        value = acc_ref[:, :, (place_ref[0] - s) & 3].reshape(256, 128).astype(BF16)
        rows = [f_ref[c, s] for f_ref in (f0_ref, f1_ref, f2_ref, f3_ref) for c in range(2)]
        total = total + dot(jnp.concatenate(rows, axis=0), value)
        if s == 0:
            mine = value
    total = total.astype(BF16)
    for s in range(4):
        for c in range(2):
            t = ((place_ref[1] - s) & 3) * 2 + ((place_ref[2] + c) & 1)
            k = (s * 2 + c) * 64
            part_ref[t] = total[k : k + 64]
    perm = by_rest()
    dv_ref[...] = dot(perm, mine, ((0,), (0,))).astype(BF16)
    dk_ref[...] = dot(perm, got[:, 256:].reshape(256, 128).astype(BF16), ((0,), (0,))).astype(BF16)


VM = pl.BlockSpec(memory_space=pltpu.VMEM)
SM = pl.BlockSpec(memory_space=pltpu.SMEM)


def call(kernel, out, specs, *args, scratch=()):
    args = [pltpu.with_memory_space_constraint(a, pltpu.VMEM) if s is VM else a for a, s in zip(args, specs)]
    return pl.pallas_call(
        kernel,
        out_shape=jax.tree.map(lambda o: pltpu.VMEM(o.shape, o.dtype), out),
        in_specs=specs,
        out_specs=jax.tree.map(lambda _: VM, out),
        scratch_shapes=scratch,
    )(*args)


def shape(*dims, dtype=BF16):
    return jax.ShapeDtypeStruct(dims, dtype)


def exchange(x, axis):
    return lax.all_to_all(x, axis, split_axis=0, concat_axis=0, tiled=True)


def shift(x, axis, by):
    size = lax.axis_size(axis)
    return lax.ppermute(x, axis, [(n, (n + by) % size) for n in range(size)])


def body(queries, keys, values, log_sums, out_grad, chosen, normed):
    rows = queries.shape[0]
    base = ((lax.axis_index("z") * 4 + lax.axis_index("y")) & 7) * 16
    base = base.astype(jnp.int32).reshape(1)
    place = jnp.stack([lax.axis_index("y"), lax.axis_index("x"), lax.axis_index("c")]).astype(jnp.int32)
    pieces = call(pack_kernel, shape(1024, 128), [SM, SM, VM, VM], base, chosen, keys, values)
    pieces = exchange(pieces.reshape(64, 16, 128), KV)
    turned = call(turn_kernel, shape(4, 64, 256), [SM, VM], place, normed)
    features = jnp.stack([turned[0]] + [shift(turned[s], "y", s) for s in range(1, 4)])
    features = jnp.stack([features, shift(features, "c", 1)])
    features = [features] + [shift(features, "x", s) for s in range(1, 4)]
    picked, ids = call(
        select_kernel, (shape(1024, 128), shape(8, 128, dtype=F32)), [VM], pieces.reshape(1024, 128)
    )
    picked = exchange(picked.reshape(64, 16, 128), KV)
    query_grad, back, own = call(
        attend_kernel,
        (shape(rows, 128), shape(64, 16, 128), shape(4, 2, 64, 128)),
        [SM, SM] + [VM] * 6,
        place, chosen, queries, keys, values, out_grad, log_sums, picked,
    )
    own = [own[0]] + [shift(own[s], "y", s) for s in range(1, 4)]
    back = exchange(back, KV)
    sums = call(gather_kernel, shape(512, 128), [VM, VM], ids, back.reshape(1024, 128))
    sums = exchange(sums.reshape(16, 32, 128), "z")
    sums = call(
        add_kernel,
        shape(4, 320, 128),
        [SM] + [VM] * 5,
        place, sums, *own,
        scratch=[pltpu.VMEM((2, 8, 4, 8, 128), F32)],
    )
    sums = exchange(sums, "y")
    key_grad, value_grad, part = call(
        finish_kernel,
        (shape(rows, 128), shape(rows, 128), shape(8, 64, 128)),
        [SM] + [VM] * 5,
        place, sums, *features,
        scratch=[pltpu.VMEM((4, 8, 4, 8, 128), F32)],
    )
    weight_grad = exchange(part.reshape(16, 32, 128), "z").astype(F32).sum(axis=0)
    return query_grad, key_grad, value_grad, weight_grad


def solution(mesh):
    fine = Mesh(mesh.devices.reshape(16, 4, 4, 2), ("z", "y", "x", "c"))
    both = P(KV, ("x", "c"))
    in_specs = (both, both, both, P(("x", "c"), KV), both, P(KV, None), both)
    return jax.shard_map(body, mesh=fine, in_specs=in_specs, out_specs=(both,) * 4, check_vma=False)
```

```python
import jax
import jax.numpy as jnp
from jax import lax
from jax.experimental import pallas as pl
from jax.experimental.pallas import tpu as pltpu
from jax.sharding import Mesh
from jax.sharding import PartitionSpec as P


KV = ("z", "y")
QB = 128
KB = 32
HD = 64
SEL = 8
F32 = jnp.float32
BF16 = jnp.bfloat16


def iota(shape, dim):
    return lax.broadcasted_iota(jnp.int32, shape, dim)


def dot(a, b, dims=((1,), (0,))):
    return lax.dot_general(a, b, (dims, ((), ())), preferred_element_type=F32)


def one_hot(hits):
    return jnp.where(hits, 1.0, 0.0).astype(BF16)


def pack_kernel(base_ref, chosen_ref, keys_ref, values_ref, normed_ref, out_ref):
    lane = iota((1, 128), 1)
    high = jnp.zeros((1, 128), F32)
    low = jnp.zeros((1, 128), F32)
    for g in range(2):
        for s in range(SEL):
            entry = chosen_ref[g, s] + 1
            here = lane == base_ref[0] + (g * SEL + s)
            high = jnp.where(here, (entry >> 3).astype(F32), high)
            low = jnp.where(here, (entry & 7).astype(F32), low)
    row, col = iota((64 * 18, 512), 0), iota((64 * 18, 512), 1)
    piece = (row * 3641) >> 16
    kind = row - piece * 18
    source = jnp.where(kind < 8, kind * KB, 256 + (kind - 10) * KB) + (piece >> 1)
    perm = one_hot(((kind < 8) | (kind >= 10)) & (col == source))
    pairs = jnp.concatenate([keys_ref[...], values_ref[...]], axis=1)
    both = dot(perm, jnp.concatenate([pairs, normed_ref[...]], axis=0))
    row = iota((64 * 18, 128), 0)
    piece = (row * 3641) >> 16
    kind = row - piece * 18
    extra = jnp.where(kind == 8, high, 0.0) + jnp.where(kind == 9, low, 0.0)
    out_ref[...] = (jnp.where((piece & 1) == 0, both[:, :128], both[:, 128:]) + extra).astype(BF16)


def select_kernel(got_ref, out_ref, ids_ref):
    got = got_ref[...]
    group, col = iota((8, 64 * 18), 0) * 144, iota((8, 64 * 18), 1)
    kind = col - ((col * 3641) >> 16) * 18
    inside = (col >= group) & (col < group + 144)
    ids = dot(one_hot(inside & (kind == 8)), got) * 8.0 + dot(one_hot(inside & (kind == 9)), got)
    ids_ref[...] = ids
    entry = ids.astype(jnp.int32) - 1
    columns = jnp.where(entry >= 0, entry + (entry >> 3) * 10, -1).astype(F32).T
    number = iota((128, 64 * 18), 1).astype(F32)
    for j in range(8):
        hot = one_hot(number == columns[:, j : j + 1])
        out_ref[j * 128 : (j + 1) * 128, :] = dot(hot, got).astype(BF16)


def half_kernel(got_ref, out_ref):
    row, col = iota((512, 64 * 18), 0), iota((512, 64 * 18), 1)
    out_ref[...] = dot(one_hot(col == row + (row >> 3) * 10 + 10), got_ref[...]).astype(BF16)


def turn_kernel(place_ref, mine_ref, other_ref, normed_ref, out_ref):
    eye = one_hot(iota((512, 512), 0) == iota((512, 512), 1))
    half = place_ref[0] & 1
    out_ref[half, :, 256:] = dot(mine_ref[...], eye, ((0,), (0,))).astype(BF16)
    out_ref[1 - half, :, 256:] = dot(other_ref[...], eye, ((0,), (0,))).astype(BF16)
    out_ref[:, :, :256] = dot(normed_ref[...], eye[:256, :256], ((0,), (0,))).astype(BF16).reshape(2, 128, 256)


def attend_kernel(
    chosen_ref, queries_ref, keys_ref, values_ref, grad_ref, sums_ref, got_ref, dq_ref, back_ref, own_ref
):
    mine = (iota((2 * QB, 128), 1) >= HD) == (iota((2 * QB, 128), 0) >= QB)
    causal = iota((QB, 2 * QB), 0) <= (iota((QB, 2 * QB), 1) & (QB - 1))
    sub = iota((SEL, 2 * QB), 0)
    low_lanes = iota((QB, 128), 1) < HD
    for g in range(2):
        span = slice(g * QB, (g + 1) * QB)
        picked = []
        for n in range(2):
            got = got_ref[:, n].astype(F32)[:, g * SEL : (g + 1) * SEL, :]
            picked.append(got.reshape(KB * SEL, 128).astype(BF16))
        keys = jnp.concatenate([picked[0], keys_ref[span, :]], axis=0)
        values = jnp.concatenate([picked[1], values_ref[span, :]], axis=0)
        q = queries_ref[span, :].astype(F32) * (HD**-0.5)
        do = grad_ref[span, :].astype(F32)
        q = jnp.where(mine, jnp.concatenate([q, q], axis=0), 0.0).astype(BF16)
        do = jnp.where(mine, jnp.concatenate([do, do], axis=0), 0.0).astype(BF16)
        sums = jnp.concatenate([sums_ref[0:1, span], sums_ref[1:2, span]], axis=1)
        used = jnp.zeros((SEL, 2 * QB), jnp.int32)
        for s in range(SEL):
            used = jnp.where(sub == s, chosen_ref[g, s] + 1, used)
        used = (used > 0)[None]
        scores = dot(keys, q, ((1,), (1,)))
        dots = dot(values, do, ((1,), (1,)))
        raw = jnp.exp(scores - sums)
        picked = jnp.where(used, raw[: KB * SEL].reshape(KB, SEL, 2 * QB), 0.0).reshape(KB * SEL, 2 * QB)
        weights = jnp.concatenate([picked, jnp.where(causal, raw[KB * SEL :], 0.0)], axis=0)
        low = weights.astype(BF16)
        deltas = jnp.sum(low.astype(F32) * dots, axis=0, keepdims=True)
        slopes = (weights * (dots - deltas)).astype(BF16)
        dk = dot(slopes, q)
        dv = dot(low, do)
        dq = dot(slopes, keys, ((0,), (0,)))
        back_ref[:, 0, g * SEL : (g + 1) * SEL, :] = dk[: KB * SEL].reshape(KB, SEL, 128).astype(BF16)
        back_ref[:, 1, g * SEL : (g + 1) * SEL, :] = dv[: KB * SEL].reshape(KB, SEL, 128).astype(BF16)
        own_ref[0, span, :] = dk[KB * SEL :].astype(BF16)
        own_ref[1, span, :] = dv[KB * SEL :].astype(BF16)
        dq_ref[span, :] = (jnp.where(low_lanes, dq[:QB], dq[QB:]) * (HD**-0.5)).astype(BF16)


def sum_kernel(place_ref, ids_ref, got_ref, own_ref, mine_ref, other_ref, out_ref):
    number = (iota((512, 128), 0) + 1).astype(F32)
    sums = jnp.zeros((512, 128), F32)
    for j in range(8):
        hot = one_hot(number == ids_ref[j : j + 1, :])
        sums = sums + dot(hot, got_ref[j * 128 : (j + 1) * 128, :])
    held = jnp.where((place_ref[0] & 1) == 1, sums, 0.0).astype(BF16)
    value = jnp.concatenate([own_ref[1], held], axis=0)
    for c, features_ref in enumerate((mine_ref, other_ref)):
        for s in range(4):
            t = ((place_ref[1] - s) & 3) * 2 + ((place_ref[2] + c) & 1)
            part = dot(features_ref[s].reshape(256, 768), value).astype(BF16).reshape(2, 4, 32, 128)
            for zz in range(2):
                for y in range(4):
                    out_ref[y, t * 2 + zz] = part[zz, y]
    sums = sums.reshape(4, 4, 4, 8, 128)
    for y in range(4):
        out_ref[y, 16:] = sums[:, :, y].reshape(4, 32, 128).astype(BF16)


def middle_kernel(got_ref, out_ref):
    total = got_ref[0, :16].astype(F32)
    for y in range(1, 4):
        total = total + got_ref[y, :16].astype(F32)
    out_ref[:, :32] = total.astype(BF16)
    sums = [got_ref[y, 16:].astype(F32).reshape(16, 8, 128) for y in range(4)]
    out_ref[:, 32:] = jnp.concatenate(sums, axis=1).astype(BF16)


def last_kernel(got_ref, own_ref, dk_ref, dv_ref, total_ref):
    total_ref[...] = got_ref[:, :32].astype(F32).sum(axis=0)
    sums = got_ref[:, 32:].reshape(512, 128)
    row, col = iota((256, 512), 0), iota((256, 512), 1)
    first = (row & 31) * 16 + (row >> 5)
    dk_ref[...] = (dot(one_hot(col == first), sums) + own_ref[0].astype(F32)).astype(BF16)
    dv_ref[...] = (dot(one_hot(col == first + 8), sums) + own_ref[1].astype(F32)).astype(BF16)


VM = pl.BlockSpec(memory_space=pltpu.VMEM)
SM = pl.BlockSpec(memory_space=pltpu.SMEM)


def call(kernel, out, specs, *args, inputs=True, hbm=(), limit=0):
    if inputs:
        args = [pltpu.with_memory_space_constraint(a, pltpu.VMEM) if s is VM else a for a, s in zip(args, specs)]
    return pl.pallas_call(
        kernel,
        out_shape=[o if n in hbm else pltpu.VMEM(o.shape, o.dtype) for n, o in enumerate(out)],
        in_specs=specs,
        out_specs=[VM] * len(out),
        compiler_params=pltpu.CompilerParams(vmem_limit_bytes=limit << 20 if limit else None),
    )(*args)


def shape(*dims, dtype=BF16):
    return jax.ShapeDtypeStruct(dims, dtype)


def exchange(x, axis):
    return lax.all_to_all(x, axis, split_axis=0, concat_axis=0, tiled=True)


def shift(x, axis, by):
    size = lax.axis_size(axis)
    return lax.ppermute(x, axis, [(n, (n + by) % size) for n in range(size)])


def body(queries, keys, values, log_sums, out_grad, chosen, normed):
    rows = queries.shape[0]
    base = ((lax.axis_index("z") * 4 + lax.axis_index("y")) & 7) * 16
    base = base.astype(jnp.int32).reshape(1)
    place = jnp.stack([lax.axis_index("y"), lax.axis_index("x"), lax.axis_index("c")]).astype(jnp.int32)
    (pieces,) = call(
        pack_kernel, [shape(1152, 128)], [SM, SM] + [VM] * 3, base, chosen, keys, values, normed, inputs=False
    )
    pieces = exchange(pieces.reshape(64, 9, 2, 128), KV).reshape(1152, 128)
    picked, ids = call(select_kernel, [shape(1024, 128), shape(8, 128, dtype=F32)], [VM], pieces)
    picked = exchange(picked.reshape(64, 16, 128), KV)
    (half,) = call(half_kernel, [shape(512, 128)], [VM], pieces)
    other = lax.ppermute(half, "y", [(n, n ^ 1) for n in range(4)])
    (features,) = call(turn_kernel, [shape(2, 128, 768)], [SM] + [VM] * 3, place, half, other, normed)
    parts = [features]
    for s in range(1, 4):
        parts.append(shift(features, "x", s))
    features = jnp.stack(parts)
    others = shift(features, "c", 1)
    query_grad, back, own = call(
        attend_kernel,
        [shape(rows, 128), shape(KB, 2, 16, 128), shape(2, rows, 128)],
        [SM] + [VM] * 6,
        chosen, queries, keys, values, out_grad, log_sums, picked.reshape(KB, 2, 16, 128),
        hbm=(0,),
    )
    back = exchange(back.reshape(64, 16, 128), KV)
    (sums,) = call(
        sum_kernel,
        [shape(4, 20, 32, 128)],
        [SM] + [VM] * 5,
        place, ids, back.reshape(1024, 128), own, features, others,
        limit=24,
    )
    sums = exchange(sums, "y")
    (sums,) = call(middle_kernel, [shape(16, 64, 128)], [VM], sums)
    sums = exchange(sums, "z")
    key_grad, value_grad, weight_grad = call(
        last_kernel,
        [shape(rows, 128), shape(rows, 128), shape(32, 128, dtype=F32)],
        [VM] * 2,
        sums, own,
        hbm=(0, 1, 2),
    )
    return query_grad, key_grad, value_grad, weight_grad


def solution(mesh):
    fine = Mesh(mesh.devices.reshape(16, 4, 4, 2), ("z", "y", "x", "c"))
    both = P(KV, ("x", "c"))
    in_specs = (both, both, both, P(("x", "c"), KV), both, P(KV, None), both)
    return jax.shard_map(body, mesh=fine, in_specs=in_specs, out_specs=(both,) * 4, check_vma=False)
```

```python
import jax
import jax.numpy as jnp
from jax import lax
from jax.experimental import pallas as pl
from jax.experimental.pallas import tpu as pltpu
from jax.sharding import Mesh
from jax.sharding import PartitionSpec as P


KV = ("z", "y")
QB = 128
KB = 32
HD = 64
SEL = 8
F32 = jnp.float32
BF16 = jnp.bfloat16


def iota(shape, dim):
    return lax.broadcasted_iota(jnp.int32, shape, dim)


def dot(a, b, dims=((1,), (0,))):
    return lax.dot_general(a, b, (dims, ((), ())), preferred_element_type=F32)


def one_hot(hits):
    return jnp.where(hits, 1.0, 0.0).astype(BF16)


def pack_kernel(base_ref, chosen_ref, keys_ref, values_ref, normed_ref, out_ref):
    lane = iota((1, 128), 1)
    high = jnp.zeros((1, 128), F32)
    low = jnp.zeros((1, 128), F32)
    for g in range(2):
        for s in range(SEL):
            entry = chosen_ref[g, s] + 1
            here = lane == base_ref[0] + (g * SEL + s)
            high = jnp.where(here, (entry >> 3).astype(F32), high)
            low = jnp.where(here, (entry & 7).astype(F32), low)
    row, col = iota((64 * 18, 512), 0), iota((64 * 18, 512), 1)
    piece = (row * 3641) >> 16
    kind = row - piece * 18
    source = jnp.where(kind < 8, kind * KB, 256 + (kind - 10) * KB) + (piece >> 1)
    perm = one_hot(((kind < 8) | (kind >= 10)) & (col == source))
    pairs = jnp.concatenate([keys_ref[...], values_ref[...]], axis=1)
    both = dot(perm, jnp.concatenate([pairs, normed_ref[...]], axis=0))
    row = iota((64 * 18, 128), 0)
    piece = (row * 3641) >> 16
    kind = row - piece * 18
    extra = jnp.where(kind == 8, high, 0.0) + jnp.where(kind == 9, low, 0.0)
    out_ref[...] = (jnp.where((piece & 1) == 0, both[:, :128], both[:, 128:]) + extra).astype(BF16)


def select_kernel(got_ref, out_ref, ids_ref):
    got = got_ref[...]
    group, col = iota((8, 64 * 18), 0) * 144, iota((8, 64 * 18), 1)
    kind = col - ((col * 3641) >> 16) * 18
    inside = (col >= group) & (col < group + 144)
    ids = dot(one_hot(inside & (kind == 8)), got) * 8.0 + dot(one_hot(inside & (kind == 9)), got)
    ids_ref[...] = ids
    entry = ids.astype(jnp.int32) - 1
    columns = jnp.where(entry >= 0, entry + (entry >> 3) * 10, -1).astype(F32).T
    number = iota((128, 64 * 18), 1).astype(F32)
    for j in range(8):
        hot = one_hot(number == columns[:, j : j + 1])
        out_ref[j * 128 : (j + 1) * 128, :] = dot(hot, got).astype(BF16)


def half_kernel(got_ref, out_ref):
    row, col = iota((512, 64 * 18), 0), iota((512, 64 * 18), 1)
    out_ref[...] = dot(one_hot(col == row + (row >> 3) * 10 + 10), got_ref[...]).astype(BF16)


def turn_own_kernel(normed_ref, out_ref):
    eye = one_hot(iota((256, 256), 0) == iota((256, 256), 1))
    out_ref[...] = dot(normed_ref[...], eye, ((0,), (0,))).astype(BF16)


def turn_kernel(y_ref, mine_ref, other_ref, own_ref, out_ref):
    eye = one_hot(iota((512, 512), 0) == iota((512, 512), 1))
    half = y_ref[0] & 1
    out_ref[half, :, 256:] = dot(mine_ref[...], eye, ((0,), (0,))).astype(BF16)
    out_ref[1 - half, :, 256:] = dot(other_ref[...], eye, ((0,), (0,))).astype(BF16)
    out_ref[:, :, :256] = own_ref[...].reshape(2, 128, 256)


def attend_kernel(
    chosen_ref, queries_ref, keys_ref, values_ref, grad_ref, sums_ref, got_ref, dq_ref, back_ref, own_ref
):
    mine = (iota((2 * QB, 128), 1) >= HD) == (iota((2 * QB, 128), 0) >= QB)
    causal = iota((QB, 2 * QB), 0) <= (iota((QB, 2 * QB), 1) & (QB - 1))
    sub = iota((SEL, 2 * QB), 0)
    low_lanes = iota((QB, 128), 1) < HD
    for g in range(2):
        span = slice(g * QB, (g + 1) * QB)
        picked = []
        for n in range(2):
            got = got_ref[:, n].astype(F32)[:, g * SEL : (g + 1) * SEL, :]
            picked.append(got.reshape(KB * SEL, 128).astype(BF16))
        keys = jnp.concatenate([picked[0], keys_ref[span, :]], axis=0)
        values = jnp.concatenate([picked[1], values_ref[span, :]], axis=0)
        q = queries_ref[span, :].astype(F32) * (HD**-0.5)
        do = grad_ref[span, :].astype(F32)
        q = jnp.where(mine, jnp.concatenate([q, q], axis=0), 0.0).astype(BF16)
        do = jnp.where(mine, jnp.concatenate([do, do], axis=0), 0.0).astype(BF16)
        sums = jnp.concatenate([sums_ref[0:1, span], sums_ref[1:2, span]], axis=1)
        used = jnp.zeros((SEL, 2 * QB), jnp.int32)
        for s in range(SEL):
            used = jnp.where(sub == s, chosen_ref[g, s] + 1, used)
        used = (used > 0)[None]
        scores = dot(keys, q, ((1,), (1,)))
        dots = dot(values, do, ((1,), (1,)))
        raw = jnp.exp(scores - sums)
        picked = jnp.where(used, raw[: KB * SEL].reshape(KB, SEL, 2 * QB), 0.0).reshape(KB * SEL, 2 * QB)
        weights = jnp.concatenate([picked, jnp.where(causal, raw[KB * SEL :], 0.0)], axis=0)
        low = weights.astype(BF16)
        deltas = jnp.sum(low.astype(F32) * dots, axis=0, keepdims=True)
        slopes = (weights * (dots - deltas)).astype(BF16)
        dk = dot(slopes, q)
        dv = dot(low, do)
        dq = dot(slopes, keys, ((0,), (0,)))
        back_ref[:, 0, g * SEL : (g + 1) * SEL, :] = dk[: KB * SEL].reshape(KB, SEL, 128).astype(BF16)
        back_ref[:, 1, g * SEL : (g + 1) * SEL, :] = dv[: KB * SEL].reshape(KB, SEL, 128).astype(BF16)
        own_ref[0, span, :] = dk[KB * SEL :].astype(BF16)
        own_ref[1, span, :] = dv[KB * SEL :].astype(BF16)
        dq_ref[span, :] = (jnp.where(low_lanes, dq[:QB], dq[QB:]) * (HD**-0.5)).astype(BF16)


def sum_kernel(y_ref, x_ref, c_ref, ids_ref, got_ref, own_ref, mine_ref, other_ref, out_ref):
    number = (iota((512, 128), 0) + 1).astype(F32)
    sums = jnp.zeros((512, 128), F32)
    for j in range(8):
        hot = one_hot(number == ids_ref[j : j + 1, :])
        sums = sums + dot(hot, got_ref[j * 128 : (j + 1) * 128, :])
    held = jnp.where((y_ref[0] & 1) == 1, sums, 0.0).astype(BF16)
    value = jnp.concatenate([own_ref[1], held], axis=0)
    for c, features_ref in enumerate((mine_ref, other_ref)):
        for s in range(4):
            t = ((x_ref[0] - s) & 3) * 2 + ((c_ref[0] + c) & 1)
            part = dot(features_ref[s].reshape(256, 768), value).astype(BF16).reshape(2, 4, 32, 128)
            for zz in range(2):
                for y in range(4):
                    out_ref[y, t * 2 + zz] = part[zz, y]
    sums = sums.reshape(4, 4, 4, 8, 128)
    for y in range(4):
        out_ref[y, 16:] = sums[:, :, y].reshape(4, 32, 128).astype(BF16)


def middle_kernel(got_ref, out_ref):
    total = got_ref[0, :16].astype(F32)
    for y in range(1, 4):
        total = total + got_ref[y, :16].astype(F32)
    out_ref[:, :32] = total.astype(BF16)
    sums = [got_ref[y, 16:].astype(F32).reshape(16, 8, 128) for y in range(4)]
    out_ref[:, 32:] = jnp.concatenate(sums, axis=1).astype(BF16)


def last_kernel(got_ref, own_ref, dk_ref, dv_ref, total_ref):
    total_ref[...] = got_ref[:, :32].astype(F32).sum(axis=0)
    sums = got_ref[:, 32:].reshape(512, 128)
    row, col = iota((256, 512), 0), iota((256, 512), 1)
    first = (row & 31) * 16 + (row >> 5)
    dk_ref[...] = (dot(one_hot(col == first), sums) + own_ref[0].astype(F32)).astype(BF16)
    dv_ref[...] = (dot(one_hot(col == first + 8), sums) + own_ref[1].astype(F32)).astype(BF16)


VM = pl.BlockSpec(memory_space=pltpu.VMEM)
SM = pl.BlockSpec(memory_space=pltpu.SMEM)


def call(kernel, out, specs, *args, inputs=True, hbm=(), limit=0):
    if inputs:
        args = [pltpu.with_memory_space_constraint(a, pltpu.VMEM) if s is VM else a for a, s in zip(args, specs)]
    return pl.pallas_call(
        kernel,
        out_shape=[o if n in hbm else pltpu.VMEM(o.shape, o.dtype) for n, o in enumerate(out)],
        in_specs=specs,
        out_specs=[VM] * len(out),
        compiler_params=pltpu.CompilerParams(vmem_limit_bytes=limit << 20 if limit else None),
    )(*args)


def shape(*dims, dtype=BF16):
    return jax.ShapeDtypeStruct(dims, dtype)


def exchange(x, axis):
    return lax.all_to_all(x, axis, split_axis=0, concat_axis=0, tiled=True)


def shift(x, axis, by):
    size = lax.axis_size(axis)
    return lax.ppermute(x, axis, [(n, (n + by) % size) for n in range(size)])


def body(queries, keys, values, log_sums, out_grad, chosen, normed):
    rows = queries.shape[0]
    base = ((lax.axis_index("z") * 4 + lax.axis_index("y")) & 7) * 16
    base = base.astype(jnp.int32).reshape(1)
    at_y, at_x, at_c = (lax.axis_index(axis).astype(jnp.int32).reshape(1) for axis in ("y", "x", "c"))
    (pieces,) = call(
        pack_kernel, [shape(1152, 128)], [SM, SM] + [VM] * 3, base, chosen, keys, values, normed, inputs=False
    )
    pieces = exchange(pieces.reshape(64, 9, 2, 128), KV).reshape(1152, 128)
    picked, ids = call(select_kernel, [shape(1024, 128), shape(8, 128, dtype=F32)], [VM], pieces)
    picked = exchange(picked.reshape(64, 16, 128), KV)
    (half,) = call(half_kernel, [shape(512, 128)], [VM], pieces)
    other = lax.ppermute(half, "y", [(n, n ^ 1) for n in range(4)])
    (turned,) = call(turn_own_kernel, [shape(256, 256)], [VM], normed)
    (features,) = call(turn_kernel, [shape(2, 128, 768)], [SM] + [VM] * 3, at_y, half, other, turned)
    parts = [features]
    for s in range(1, 4):
        parts.append(shift(features, "x", s))
    features = jnp.stack(parts)
    others = shift(features, "c", 1)
    query_grad, back, own = call(
        attend_kernel,
        [shape(rows, 128), shape(KB, 2, 16, 128), shape(2, rows, 128)],
        [SM] + [VM] * 6,
        chosen, queries, keys, values, out_grad, log_sums, picked.reshape(KB, 2, 16, 128),
        hbm=(0,),
    )
    back = exchange(back.reshape(64, 16, 128), KV)
    (sums,) = call(
        sum_kernel,
        [shape(4, 20, 32, 128)],
        [SM] * 3 + [VM] * 5,
        at_y, at_x, at_c, ids, back.reshape(1024, 128), own, features, others,
        limit=24,
    )
    sums = exchange(sums, "y")
    (sums,) = call(middle_kernel, [shape(16, 64, 128)], [VM], sums)
    sums = exchange(sums, "z")
    key_grad, value_grad, weight_grad = call(
        last_kernel,
        [shape(rows, 128), shape(rows, 128), shape(32, 128, dtype=F32)],
        [VM] * 2,
        sums, own,
        hbm=(0, 1, 2),
    )
    return query_grad, key_grad, value_grad, weight_grad


def solution(mesh):
    fine = Mesh(mesh.devices.reshape(16, 4, 4, 2), ("z", "y", "x", "c"))
    both = P(KV, ("x", "c"))
    in_specs = (both, both, both, P(("x", "c"), KV), both, P(KV, None), both)
    return jax.shard_map(body, mesh=fine, in_specs=in_specs, out_specs=(both,) * 4, check_vma=False)
```

```python
import jax
import jax.numpy as jnp
from jax import lax
from jax.experimental import pallas as pl
from jax.experimental.pallas import tpu as pltpu
from jax.sharding import Mesh
from jax.sharding import PartitionSpec as P


KV = ("z", "y")
QB = 128
KB = 32
HD = 64
SEL = 8
F32 = jnp.float32
BF16 = jnp.bfloat16


def iota(shape, dim):
    return lax.broadcasted_iota(jnp.int32, shape, dim)


def dot(a, b, dims=((1,), (0,))):
    return lax.dot_general(a, b, (dims, ((), ())), preferred_element_type=F32)


def one_hot(hits):
    return jnp.where(hits, 1.0, 0.0).astype(BF16)


def pack_kernel(base_ref, chosen_ref, keys_ref, values_ref, normed_ref, out_ref):
    lane = iota((1, 128), 1)
    high = jnp.zeros((1, 128), F32)
    low = jnp.zeros((1, 128), F32)
    for g in range(2):
        for s in range(SEL):
            entry = chosen_ref[g, s] + 1
            here = lane == base_ref[0] + (g * SEL + s)
            high = jnp.where(here, (entry >> 3).astype(F32), high)
            low = jnp.where(here, (entry & 7).astype(F32), low)
    row, col = iota((64 * 18, 512), 0), iota((64 * 18, 512), 1)
    piece = (row * 3641) >> 16
    kind = row - piece * 18
    source = jnp.where(kind < 8, kind * KB, 256 + (kind - 10) * KB) + (piece >> 1)
    perm = one_hot(((kind < 8) | (kind >= 10)) & (col == source))
    pairs = jnp.concatenate([keys_ref[...], values_ref[...]], axis=1)
    both = dot(perm, jnp.concatenate([pairs, normed_ref[...]], axis=0))
    row = iota((64 * 18, 128), 0)
    piece = (row * 3641) >> 16
    kind = row - piece * 18
    extra = jnp.where(kind == 8, high, 0.0) + jnp.where(kind == 9, low, 0.0)
    out_ref[...] = (jnp.where((piece & 1) == 0, both[:, :128], both[:, 128:]) + extra).astype(BF16)


def select_kernel(got_ref, out_ref, ids_ref):
    got = got_ref[...]
    group, col = iota((8, 64 * 18), 0) * 144, iota((8, 64 * 18), 1)
    kind = col - ((col * 3641) >> 16) * 18
    inside = (col >= group) & (col < group + 144)
    ids = dot(one_hot(inside & (kind == 8)), got) * 8.0 + dot(one_hot(inside & (kind == 9)), got)
    ids_ref[...] = ids
    entry = ids.astype(jnp.int32) - 1
    columns = jnp.where(entry >= 0, entry + (entry >> 3) * 10, -1).astype(F32).T
    number = iota((128, 64 * 18), 1).astype(F32)
    for j in range(8):
        hot = one_hot(number == columns[:, j : j + 1])
        out_ref[j * 128 : (j + 1) * 128, :] = dot(hot, got).astype(BF16)


def half_kernel(y_ref, got_ref, normed_ref, mine_ref, sent_ref):
    row, col = iota((512, 64 * 18), 0), iota((512, 64 * 18), 1)
    mine = dot(one_hot(col == row + (row >> 3) * 10 + 10), got_ref[...])
    mine_ref[...] = mine.astype(BF16)
    normed = normed_ref[...].astype(F32)
    normed = jnp.concatenate([normed[:, :128], normed[:, 128:]], axis=0)
    sent_ref[...] = jnp.where((y_ref[0] & 1) == 1, normed, mine).astype(BF16)


def turn_kernel(y_ref, mine_ref, other_ref, normed_ref, out_ref):
    eye = one_hot(iota((512, 512), 0) == iota((512, 512), 1))
    other = other_ref[...].astype(F32)
    normed = normed_ref[...].astype(F32)
    for n in range(2):
        kept = other if n == 0 else mine_ref[...].astype(F32)
        owned = jnp.concatenate([normed[:, n * 128 : (n + 1) * 128], other[n * 256 : (n + 1) * 256]], axis=0)
        part = jnp.where((y_ref[0] & 1) == 1, kept, owned).astype(BF16)
        out_ref[n] = dot(part, eye, ((0,), (0,))).astype(BF16)


def attend_kernel(
    chosen_ref, queries_ref, keys_ref, values_ref, grad_ref, sums_ref, got_ref, dq_ref, back_ref, own_ref
):
    mine = (iota((2 * QB, 128), 1) >= HD) == (iota((2 * QB, 128), 0) >= QB)
    causal = iota((QB, 2 * QB), 0) <= (iota((QB, 2 * QB), 1) & (QB - 1))
    sub = iota((SEL, 2 * QB), 0)
    low_lanes = iota((QB, 128), 1) < HD
    for g in range(2):
        span = slice(g * QB, (g + 1) * QB)
        picked = []
        for n in range(2):
            got = got_ref[:, n].astype(F32)[:, g * SEL : (g + 1) * SEL, :]
            picked.append(got.reshape(KB * SEL, 128).astype(BF16))
        keys = jnp.concatenate([picked[0], keys_ref[span, :]], axis=0)
        values = jnp.concatenate([picked[1], values_ref[span, :]], axis=0)
        q = queries_ref[span, :].astype(F32) * (HD**-0.5)
        do = grad_ref[span, :].astype(F32)
        q = jnp.where(mine, jnp.concatenate([q, q], axis=0), 0.0).astype(BF16)
        do = jnp.where(mine, jnp.concatenate([do, do], axis=0), 0.0).astype(BF16)
        sums = jnp.concatenate([sums_ref[0:1, span], sums_ref[1:2, span]], axis=1)
        used = jnp.zeros((SEL, 2 * QB), jnp.int32)
        for s in range(SEL):
            used = jnp.where(sub == s, chosen_ref[g, s] + 1, used)
        used = (used > 0)[None]
        scores = dot(keys, q, ((1,), (1,)))
        dots = dot(values, do, ((1,), (1,)))
        raw = jnp.exp(scores - sums)
        picked = jnp.where(used, raw[: KB * SEL].reshape(KB, SEL, 2 * QB), 0.0).reshape(KB * SEL, 2 * QB)
        weights = jnp.concatenate([picked, jnp.where(causal, raw[KB * SEL :], 0.0)], axis=0)
        low = weights.astype(BF16)
        deltas = jnp.sum(low.astype(F32) * dots, axis=0, keepdims=True)
        slopes = (weights * (dots - deltas)).astype(BF16)
        dk = dot(slopes, q)
        dv = dot(low, do)
        dq = dot(slopes, keys, ((0,), (0,)))
        back_ref[:, 0, g * SEL : (g + 1) * SEL, :] = dk[: KB * SEL].reshape(KB, SEL, 128).astype(BF16)
        back_ref[:, 1, g * SEL : (g + 1) * SEL, :] = dv[: KB * SEL].reshape(KB, SEL, 128).astype(BF16)
        own_ref[0, span, :] = dk[KB * SEL :].astype(BF16)
        own_ref[1, span, :] = dv[KB * SEL :].astype(BF16)
        dq_ref[span, :] = (jnp.where(low_lanes, dq[:QB], dq[QB:]) * (HD**-0.5)).astype(BF16)


def sum_kernel(y_ref, x_ref, c_ref, ids_ref, got_ref, own_ref, partner_ref, mine_ref, other_ref, out_ref):
    number = (iota((512, 128), 0) + 1).astype(F32)
    sums = jnp.zeros((512, 128), F32)
    for j in range(8):
        hot = one_hot(number == ids_ref[j : j + 1, :])
        sums = sums + dot(hot, got_ref[j * 128 : (j + 1) * 128, :])
    owned = jnp.concatenate([own_ref[1], partner_ref[...]], axis=0).astype(F32)
    value = jnp.where((y_ref[0] & 1) == 1, sums, owned).astype(BF16)
    for c, features_ref in enumerate((mine_ref, other_ref)):
        for s in range(4):
            t = ((x_ref[0] - s) & 3) * 2 + ((c_ref[0] + c) & 1)
            part = dot(features_ref[s].reshape(256, 512), value).astype(BF16).reshape(2, 4, 32, 128)
            for zz in range(2):
                for y in range(4):
                    out_ref[y, t * 2 + zz] = part[zz, y]
    sums = sums.reshape(4, 4, 4, 8, 128)
    for y in range(4):
        out_ref[y, 16:] = sums[:, :, y].reshape(4, 32, 128).astype(BF16)


def middle_kernel(got_ref, out_ref):
    total = got_ref[0, :16].astype(F32)
    for y in range(1, 4):
        total = total + got_ref[y, :16].astype(F32)
    out_ref[:, :32] = total.astype(BF16)
    sums = [got_ref[y, 16:].astype(F32).reshape(16, 8, 128) for y in range(4)]
    out_ref[:, 32:] = jnp.concatenate(sums, axis=1).astype(BF16)


def last_kernel(got_ref, own_ref, dk_ref, dv_ref, total_ref):
    total_ref[...] = got_ref[:, :32].astype(F32).sum(axis=0)
    sums = got_ref[:, 32:].reshape(512, 128)
    row, col = iota((256, 512), 0), iota((256, 512), 1)
    first = (row & 31) * 16 + (row >> 5)
    dk_ref[...] = (dot(one_hot(col == first), sums) + own_ref[0].astype(F32)).astype(BF16)
    dv_ref[...] = (dot(one_hot(col == first + 8), sums) + own_ref[1].astype(F32)).astype(BF16)


VM = pl.BlockSpec(memory_space=pltpu.VMEM)
SM = pl.BlockSpec(memory_space=pltpu.SMEM)


def call(kernel, out, specs, *args, inputs=True, hbm=(), limit=0):
    if inputs:
        args = [pltpu.with_memory_space_constraint(a, pltpu.VMEM) if s is VM else a for a, s in zip(args, specs)]
    return pl.pallas_call(
        kernel,
        out_shape=[o if n in hbm else pltpu.VMEM(o.shape, o.dtype) for n, o in enumerate(out)],
        in_specs=specs,
        out_specs=[VM] * len(out),
        compiler_params=pltpu.CompilerParams(vmem_limit_bytes=limit << 20 if limit else None),
    )(*args)


def shape(*dims, dtype=BF16):
    return jax.ShapeDtypeStruct(dims, dtype)


def exchange(x, axis):
    return lax.all_to_all(x, axis, split_axis=0, concat_axis=0, tiled=True)


def shift(x, axis, by):
    size = lax.axis_size(axis)
    return lax.ppermute(x, axis, [(n, (n + by) % size) for n in range(size)])


def swapped(x):
    return lax.ppermute(x, "y", [(n, n ^ 1) for n in range(4)])


def body(queries, keys, values, log_sums, out_grad, chosen, normed):
    rows = queries.shape[0]
    base = ((lax.axis_index("z") * 4 + lax.axis_index("y")) & 7) * 16
    base = base.astype(jnp.int32).reshape(1)
    at_y, at_x, at_c = (lax.axis_index(axis).astype(jnp.int32).reshape(1) for axis in ("y", "x", "c"))
    (pieces,) = call(
        pack_kernel, [shape(1152, 128)], [SM, SM] + [VM] * 3, base, chosen, keys, values, normed, inputs=False
    )
    pieces = exchange(pieces.reshape(64, 9, 2, 128), KV).reshape(1152, 128)
    picked, ids = call(select_kernel, [shape(1024, 128), shape(8, 128, dtype=F32)], [VM], pieces)
    picked = exchange(picked.reshape(64, 16, 128), KV)
    half, sent = call(half_kernel, [shape(512, 128)] * 2, [SM] + [VM] * 2, at_y, pieces, normed)
    other = swapped(sent)
    (features,) = call(turn_kernel, [shape(2, 128, 512)], [SM] + [VM] * 3, at_y, half, other, normed)
    parts = [features]
    for s in range(1, 4):
        parts.append(shift(features, "x", s))
    features = jnp.stack(parts)
    others = shift(features, "c", 1)
    query_grad, back, own = call(
        attend_kernel,
        [shape(rows, 128), shape(KB, 2, 16, 128), shape(2, rows, 128)],
        [SM] + [VM] * 6,
        chosen, queries, keys, values, out_grad, log_sums, picked.reshape(KB, 2, 16, 128),
        hbm=(0,),
    )
    back = exchange(back.reshape(64, 16, 128), KV)
    partner = swapped(own[1])
    (sums,) = call(
        sum_kernel,
        [shape(4, 20, 32, 128)],
        [SM] * 3 + [VM] * 6,
        at_y, at_x, at_c, ids, back.reshape(1024, 128), own, partner, features, others,
        limit=24,
    )
    sums = exchange(sums, "y")
    (sums,) = call(middle_kernel, [shape(16, 64, 128)], [VM], sums)
    sums = exchange(sums, "z")
    key_grad, value_grad, weight_grad = call(
        last_kernel,
        [shape(rows, 128), shape(rows, 128), shape(32, 128, dtype=F32)],
        [VM] * 2,
        sums, own,
        hbm=(0, 1, 2),
    )
    return query_grad, key_grad, value_grad, weight_grad


def solution(mesh):
    fine = Mesh(mesh.devices.reshape(16, 4, 4, 2), ("z", "y", "x", "c"))
    both = P(KV, ("x", "c"))
    in_specs = (both, both, both, P(("x", "c"), KV), both, P(KV, None), both)
    return jax.shard_map(body, mesh=fine, in_specs=in_specs, out_specs=(both,) * 4, check_vma=False)
```

```python
import jax
import jax.numpy as jnp
from jax import lax
from jax.experimental import pallas as pl
from jax.experimental.pallas import tpu as pltpu
from jax.sharding import Mesh
from jax.sharding import PartitionSpec as P


KV = ("z", "y")
QB = 128
KB = 32
HD = 64
SEL = 8
F32 = jnp.float32
BF16 = jnp.bfloat16


def iota(shape, dim):
    return lax.broadcasted_iota(jnp.int32, shape, dim)


def dot(a, b, dims=((1,), (0,))):
    return lax.dot_general(a, b, (dims, ((), ())), preferred_element_type=F32)


def one_hot(hits):
    return jnp.where(hits, 1.0, 0.0).astype(BF16)


def pack_kernel(base_ref, chosen_ref, keys_ref, values_ref, normed_ref, out_ref):
    lane = iota((1, 128), 1)
    high = jnp.zeros((1, 128), F32)
    low = jnp.zeros((1, 128), F32)
    for g in range(2):
        for s in range(SEL):
            entry = chosen_ref[g, s] + 1
            here = lane == base_ref[0] + (g * SEL + s)
            high = jnp.where(here, (entry >> 3).astype(F32), high)
            low = jnp.where(here, (entry & 7).astype(F32), low)
    row, col = iota((64 * 18, 512), 0), iota((64 * 18, 512), 1)
    piece = (row * 3641) >> 16
    kind = row - piece * 18
    source = jnp.where(kind < 8, kind * KB, 256 + (kind - 10) * KB) + (piece >> 1)
    perm = one_hot(((kind < 8) | (kind >= 10)) & (col == source))
    pairs = jnp.concatenate([keys_ref[...], values_ref[...]], axis=1)
    both = dot(perm, jnp.concatenate([pairs, normed_ref[...]], axis=0))
    row = iota((64 * 18, 128), 0)
    piece = (row * 3641) >> 16
    kind = row - piece * 18
    extra = jnp.where(kind == 8, high, 0.0) + jnp.where(kind == 9, low, 0.0)
    out_ref[...] = (jnp.where((piece & 1) == 0, both[:, :128], both[:, 128:]) + extra).astype(BF16)


def select_kernel(got_ref, meta_ref, out_ref, ids_ref):
    got = got_ref[...]
    meta = meta_ref[...]
    group, col = iota((8, 128), 0) * 16, iota((8, 128), 1)
    inside = (col >= group) & (col < group + 16)
    even = (col & 1) == 0
    ids = dot(one_hot(inside & even), meta) * 8.0 + dot(one_hot(inside & ~even), meta)
    ids_ref[...] = ids
    columns = ids.T
    number = (iota((128, 512), 1) + 1).astype(F32)
    for j in range(8):
        hot = one_hot(number == columns[:, j : j + 1])
        out_ref[j * 128 : (j + 1) * 128, :] = dot(hot, got).astype(BF16)


def sent_kernel(y_ref, ids_ref, mine_ref, normed_ref, out_ref):
    normed = normed_ref[...].astype(F32)
    normed = jnp.concatenate([normed[:, :128], normed[:, 128:]], axis=0)
    out_ref[...] = jnp.where((y_ref[0] & 1) == 1, normed, mine_ref[...].astype(F32)).astype(BF16)


def turn_kernel(y_ref, mine_ref, other_ref, normed_ref, out_ref):
    eye = one_hot(iota((512, 512), 0) == iota((512, 512), 1))
    other = other_ref[...].astype(F32)
    normed = normed_ref[...].astype(F32)
    for n in range(2):
        kept = other if n == 0 else mine_ref[...].astype(F32)
        owned = jnp.concatenate([normed[:, n * 128 : (n + 1) * 128], other[n * 256 : (n + 1) * 256]], axis=0)
        part = jnp.where((y_ref[0] & 1) == 1, kept, owned).astype(BF16)
        out_ref[n] = dot(part, eye, ((0,), (0,))).astype(BF16)


def attend_kernel(
    chosen_ref, queries_ref, keys_ref, values_ref, grad_ref, sums_ref, got_ref, dq_ref, back_ref, own_ref
):
    mine = (iota((2 * QB, 128), 1) >= HD) == (iota((2 * QB, 128), 0) >= QB)
    causal = iota((QB, 2 * QB), 0) <= (iota((QB, 2 * QB), 1) & (QB - 1))
    sub = iota((SEL, 2 * QB), 0)
    low_lanes = iota((QB, 128), 1) < HD
    for g in range(2):
        span = slice(g * QB, (g + 1) * QB)
        picked = []
        for n in range(2):
            picked.append(got_ref[:, n, g * SEL : (g + 1) * SEL, :].reshape(KB * SEL, 128))
        keys = jnp.concatenate([picked[0], keys_ref[span, :]], axis=0)
        values = jnp.concatenate([picked[1], values_ref[span, :]], axis=0)
        q = queries_ref[span, :].astype(F32) * (HD**-0.5)
        do = grad_ref[span, :].astype(F32)
        q = jnp.where(mine, jnp.concatenate([q, q], axis=0), 0.0).astype(BF16)
        do = jnp.where(mine, jnp.concatenate([do, do], axis=0), 0.0).astype(BF16)
        sums = jnp.concatenate([sums_ref[0:1, span], sums_ref[1:2, span]], axis=1)
        used = jnp.zeros((SEL, 2 * QB), jnp.int32)
        for s in range(SEL):
            used = jnp.where(sub == s, chosen_ref[g, s] + 1, used)
        used = (used > 0)[None]
        scores = dot(keys, q, ((1,), (1,)))
        dots = dot(values, do, ((1,), (1,)))
        raw = jnp.exp(scores - sums)
        picked = jnp.where(used, raw[: KB * SEL].reshape(KB, SEL, 2 * QB), 0.0).reshape(KB * SEL, 2 * QB)
        weights = jnp.concatenate([picked, jnp.where(causal, raw[KB * SEL :], 0.0)], axis=0)
        low = weights.astype(BF16)
        deltas = jnp.sum(low.astype(F32) * dots, axis=0, keepdims=True)
        slopes = (weights * (dots - deltas)).astype(BF16)
        dk = dot(slopes, q)
        dv = dot(low, do)
        dq = dot(slopes, keys, ((0,), (0,)))
        back_ref[:, 0, g * SEL : (g + 1) * SEL, :] = dk[: KB * SEL].reshape(KB, SEL, 128).astype(BF16)
        back_ref[:, 1, g * SEL : (g + 1) * SEL, :] = dv[: KB * SEL].reshape(KB, SEL, 128).astype(BF16)
        own_ref[0, span, :] = dk[KB * SEL :].astype(BF16)
        own_ref[1, span, :] = dv[KB * SEL :].astype(BF16)
        dq_ref[span, :] = (jnp.where(low_lanes, dq[:QB], dq[QB:]) * (HD**-0.5)).astype(BF16)


def sum_kernel(y_ref, x_ref, c_ref, ids_ref, got_ref, own_ref, partner_ref, mine_ref, other_ref, out_ref):
    number = (iota((512, 128), 0) + 1).astype(F32)
    sums = jnp.zeros((512, 128), F32)
    for j in range(8):
        hot = one_hot(number == ids_ref[j : j + 1, :])
        sums = sums + dot(hot, got_ref[j * 128 : (j + 1) * 128, :])
    owned = jnp.concatenate([own_ref[1], partner_ref[...]], axis=0).astype(F32)
    value = jnp.where((y_ref[0] & 1) == 1, sums, owned).astype(BF16)
    for c, features_ref in enumerate((mine_ref, other_ref)):
        for s in range(4):
            t = ((x_ref[0] - s) & 3) * 2 + ((c_ref[0] + c) & 1)
            part = dot(features_ref[s].reshape(256, 512), value).astype(BF16).reshape(2, 4, 32, 128)
            for zz in range(2):
                for y in range(4):
                    out_ref[y, t * 2 + zz] = part[zz, y]
    sums = sums.reshape(4, 4, 4, 8, 128)
    for y in range(4):
        out_ref[y, 16:] = sums[:, :, y].reshape(4, 32, 128).astype(BF16)


def middle_kernel(got_ref, out_ref):
    total = got_ref[0, :16].astype(F32)
    for y in range(1, 4):
        total = total + got_ref[y, :16].astype(F32)
    out_ref[:, :32] = total.astype(BF16)
    sums = [got_ref[y, 16:].astype(F32).reshape(16, 8, 128) for y in range(4)]
    out_ref[:, 32:] = jnp.concatenate(sums, axis=1).astype(BF16)


def last_kernel(got_ref, own_ref, dk_ref, dv_ref, total_ref):
    total_ref[...] = got_ref[:, :32].astype(F32).sum(axis=0)
    sums = got_ref[:, 32:].reshape(512, 128)
    row, col = iota((256, 512), 0), iota((256, 512), 1)
    first = (row & 31) * 16 + (row >> 5)
    dk_ref[...] = (dot(one_hot(col == first), sums) + own_ref[0].astype(F32)).astype(BF16)
    dv_ref[...] = (dot(one_hot(col == first + 8), sums) + own_ref[1].astype(F32)).astype(BF16)


VM = pl.BlockSpec(memory_space=pltpu.VMEM)
SM = pl.BlockSpec(memory_space=pltpu.SMEM)


def call(kernel, out, specs, *args, inputs=True, hbm=(), limit=0):
    if inputs:
        args = [pltpu.with_memory_space_constraint(a, pltpu.VMEM) if s is VM else a for a, s in zip(args, specs)]
    return pl.pallas_call(
        kernel,
        out_shape=[o if n in hbm else pltpu.VMEM(o.shape, o.dtype) for n, o in enumerate(out)],
        in_specs=specs,
        out_specs=[VM] * len(out),
        compiler_params=pltpu.CompilerParams(vmem_limit_bytes=limit << 20 if limit else None),
    )(*args)


def shape(*dims, dtype=BF16):
    return jax.ShapeDtypeStruct(dims, dtype)


def exchange(x, axis):
    return lax.all_to_all(x, axis, split_axis=0, concat_axis=0, tiled=True)


def shift(x, axis, by):
    size = lax.axis_size(axis)
    return lax.ppermute(x, axis, [(n, (n + by) % size) for n in range(size)])


def swapped(x):
    return lax.ppermute(x, "y", [(n, n ^ 1) for n in range(4)])


def body(queries, keys, values, log_sums, out_grad, chosen, normed):
    rows = queries.shape[0]
    base = ((lax.axis_index("z") * 4 + lax.axis_index("y")) & 7) * 16
    base = base.astype(jnp.int32).reshape(1)
    at_y, at_x, at_c = (lax.axis_index(axis).astype(jnp.int32).reshape(1) for axis in ("y", "x", "c"))
    (pieces,) = call(
        pack_kernel, [shape(1152, 128)], [SM, SM] + [VM] * 3, base, chosen, keys, values, normed, inputs=False
    )
    pieces = exchange(pieces.reshape(64, 9, 2, 128), KV)
    table, meta, half = (pieces[:, a:b].reshape(-1, 128) for a, b in ((0, 4), (4, 5), (5, 9)))
    picked, ids = call(select_kernel, [shape(1024, 128), shape(8, 128, dtype=F32)], [VM] * 2, table, meta)
    picked = exchange(picked.reshape(64, 16, 128), KV)
    (sent,) = call(sent_kernel, [shape(512, 128)], [SM] + [VM] * 3, at_y, ids, half, normed)
    other = swapped(sent)
    (features,) = call(turn_kernel, [shape(2, 128, 512)], [SM] + [VM] * 3, at_y, half, other, normed)
    parts = [features]
    for s in range(1, 4):
        parts.append(shift(features, "x", s))
    features = jnp.stack(parts)
    others = shift(features, "c", 1)
    query_grad, back, own = call(
        attend_kernel,
        [shape(rows, 128), shape(KB, 2, 16, 128), shape(2, rows, 128)],
        [SM] + [VM] * 6,
        chosen, queries, keys, values, out_grad, log_sums, picked.reshape(KB, 2, 16, 128),
        hbm=(0,),
    )
    back = exchange(back.reshape(64, 16, 128), KV)
    partner = swapped(own[1])
    (sums,) = call(
        sum_kernel,
        [shape(4, 20, 32, 128)],
        [SM] * 3 + [VM] * 6,
        at_y, at_x, at_c, ids, back.reshape(1024, 128), own, partner, features, others,
        limit=24,
    )
    sums = exchange(sums, "y")
    (sums,) = call(middle_kernel, [shape(16, 64, 128)], [VM], sums)
    sums = exchange(sums, "z")
    key_grad, value_grad, weight_grad = call(
        last_kernel,
        [shape(rows, 128), shape(rows, 128), shape(32, 128, dtype=F32)],
        [VM] * 2,
        sums, own,
        hbm=(0, 1, 2),
    )
    return query_grad, key_grad, value_grad, weight_grad


def solution(mesh):
    fine = Mesh(mesh.devices.reshape(16, 4, 4, 2), ("z", "y", "x", "c"))
    both = P(KV, ("x", "c"))
    in_specs = (both, both, both, P(("x", "c"), KV), both, P(KV, None), both)
    return jax.shard_map(body, mesh=fine, in_specs=in_specs, out_specs=(both,) * 4, check_vma=False)
```

```python
import jax
import jax.numpy as jnp
from jax import lax
from jax.experimental import pallas as pl
from jax.experimental.pallas import tpu as pltpu
from jax.sharding import Mesh
from jax.sharding import PartitionSpec as P


KV = ("z", "y")
QB = 128
KB = 32
HD = 64
SEL = 8
F32 = jnp.float32
BF16 = jnp.bfloat16


def iota(shape, dim):
    return lax.broadcasted_iota(jnp.int32, shape, dim)


def dot(a, b, dims=((1,), (0,))):
    return lax.dot_general(a, b, (dims, ((), ())), preferred_element_type=F32)


def one_hot(hits):
    return jnp.where(hits, 1.0, 0.0).astype(BF16)


def pack_kernel(base_ref, chosen_ref, keys_ref, values_ref, normed_ref, out_ref):
    lane = iota((1, 128), 1)
    high = jnp.zeros((1, 128), F32)
    low = jnp.zeros((1, 128), F32)
    for g in range(2):
        for s in range(SEL):
            entry = chosen_ref[g, s] + 1
            here = lane == base_ref[0] + (g * SEL + s)
            high = jnp.where(here, (entry >> 3).astype(F32), high)
            low = jnp.where(here, (entry & 7).astype(F32), low)
    row = iota((64 * 18, 128), 0)
    piece = (row * 3641) >> 16
    kind = row - piece * 18
    source = jnp.where(kind < 8, kind * KB, 256 + (kind - 10) * KB) + (piece >> 1)
    source = jnp.where((kind == 8) | (kind == 9), -1, source) - iota((64 * 18, 128), 1)
    perm = jnp.concatenate([one_hot(source == n * 128) for n in range(4)], axis=1)
    pairs = jnp.concatenate([keys_ref[...], values_ref[...]], axis=1)
    both = dot(perm, jnp.concatenate([pairs, normed_ref[...]], axis=0))
    extra = jnp.where(kind == 8, high, 0.0) + jnp.where(kind == 9, low, 0.0)
    out_ref[...] = (jnp.where((piece & 1) == 0, both[:, :128], both[:, 128:]) + extra).astype(BF16)


def select_kernel(got_ref, meta_ref, out_ref, ids_ref):
    got = got_ref[...]
    meta = meta_ref[...]
    group, col = iota((8, 128), 0) * 16, iota((8, 128), 1)
    inside = (col >= group) & (col < group + 16)
    even = (col & 1) == 0
    ids = dot(one_hot(inside & even), meta) * 8.0 + dot(one_hot(inside & ~even), meta)
    ids_ref[...] = ids
    columns = ids.T
    number = (iota((128, 512), 1) + 1).astype(F32)
    hot = jnp.concatenate([one_hot(number == columns[:, j : j + 1]) for j in range(8)], axis=0)
    out_ref[...] = dot(hot, got).astype(BF16)


def sent_kernel(y_ref, ids_ref, mine_ref, normed_ref, out_ref):
    normed = normed_ref[...].astype(F32)
    normed = jnp.concatenate([normed[:, :128], normed[:, 128:]], axis=0)
    out_ref[...] = jnp.where((y_ref[0] & 1) == 1, normed, mine_ref[...].astype(F32)).astype(BF16)


def turn_kernel(y_ref, mine_ref, other_ref, normed_ref, out_ref):
    eye = one_hot(iota((512, 512), 0) == iota((512, 512), 1))
    other = other_ref[...].astype(F32)
    normed = normed_ref[...].astype(F32)
    for n in range(2):
        kept = other if n == 0 else mine_ref[...].astype(F32)
        owned = jnp.concatenate([normed[:, n * 128 : (n + 1) * 128], other[n * 256 : (n + 1) * 256]], axis=0)
        part = jnp.where((y_ref[0] & 1) == 1, kept, owned).astype(BF16)
        out_ref[n] = dot(part, eye, ((0,), (0,))).astype(BF16)


def attend_kernel(
    chosen_ref, queries_ref, keys_ref, values_ref, grad_ref, sums_ref, got_ref, dq_ref, back_ref, own_ref
):
    mine = (iota((2 * QB, 128), 1) >= HD) == (iota((2 * QB, 128), 0) >= QB)
    causal = iota((QB, 2 * QB), 0) <= (iota((QB, 2 * QB), 1) & (QB - 1))
    sub = iota((SEL, 2 * QB), 0)
    low_lanes = iota((QB, 128), 1) < HD
    for g in range(2):
        span = slice(g * QB, (g + 1) * QB)
        picked = []
        for n in range(2):
            picked.append(got_ref[:, n, g * SEL : (g + 1) * SEL, :].reshape(KB * SEL, 128))
        keys = jnp.concatenate([picked[0], keys_ref[span, :]], axis=0)
        values = jnp.concatenate([picked[1], values_ref[span, :]], axis=0)
        q = queries_ref[span, :].astype(F32) * (HD**-0.5)
        do = grad_ref[span, :].astype(F32)
        q = jnp.where(mine, jnp.concatenate([q, q], axis=0), 0.0).astype(BF16)
        do = jnp.where(mine, jnp.concatenate([do, do], axis=0), 0.0).astype(BF16)
        sums = jnp.concatenate([sums_ref[0:1, span], sums_ref[1:2, span]], axis=1)
        used = jnp.zeros((SEL, 2 * QB), jnp.int32)
        for s in range(SEL):
            used = jnp.where(sub == s, chosen_ref[g, s] + 1, used)
        used = (used > 0)[None]
        scores = dot(keys, q, ((1,), (1,)))
        dots = dot(values, do, ((1,), (1,)))
        raw = jnp.exp(scores - sums)
        picked = jnp.where(used, raw[: KB * SEL].reshape(KB, SEL, 2 * QB), 0.0).reshape(KB * SEL, 2 * QB)
        weights = jnp.concatenate([picked, jnp.where(causal, raw[KB * SEL :], 0.0)], axis=0)
        low = weights.astype(BF16)
        deltas = jnp.sum(low.astype(F32) * dots, axis=0, keepdims=True)
        slopes = (weights * (dots - deltas)).astype(BF16)
        dk = dot(slopes, q)
        dv = dot(low, do)
        dq = dot(slopes, keys, ((0,), (0,)))
        back_ref[:, 0, g * SEL : (g + 1) * SEL, :] = dk[: KB * SEL].reshape(KB, SEL, 128).astype(BF16)
        back_ref[:, 1, g * SEL : (g + 1) * SEL, :] = dv[: KB * SEL].reshape(KB, SEL, 128).astype(BF16)
        own_ref[0, span, :] = dk[KB * SEL :].astype(BF16)
        own_ref[1, span, :] = dv[KB * SEL :].astype(BF16)
        dq_ref[span, :] = (jnp.where(low_lanes, dq[:QB], dq[QB:]) * (HD**-0.5)).astype(BF16)


def sum_kernel(y_ref, x_ref, c_ref, ids_ref, got_ref, own_ref, partner_ref, mine_ref, other_ref, out_ref):
    number = (iota((512, 128), 0) + 1).astype(F32)
    hot = jnp.concatenate([one_hot(number == ids_ref[j : j + 1, :]) for j in range(8)], axis=1)
    sums = dot(hot, got_ref[...])
    owned = jnp.concatenate([own_ref[1], partner_ref[...]], axis=0).astype(F32)
    value = jnp.where((y_ref[0] & 1) == 1, sums, owned).astype(BF16)
    for c, features_ref in enumerate((mine_ref, other_ref)):
        part = dot(features_ref[...].reshape(1024, 512), value).astype(BF16).reshape(4, 2, 4, 32, 128)
        for s in range(4):
            t = ((x_ref[0] - s) & 3) * 2 + ((c_ref[0] + c) & 1)
            for zz in range(2):
                for y in range(4):
                    out_ref[y, t * 2 + zz] = part[s, zz, y]
    sums = sums.reshape(4, 4, 4, 8, 128)
    for y in range(4):
        out_ref[y, 16:] = sums[:, :, y].reshape(4, 32, 128).astype(BF16)


def middle_kernel(got_ref, out_ref):
    total = got_ref[0, :16].astype(F32)
    for y in range(1, 4):
        total = total + got_ref[y, :16].astype(F32)
    out_ref[:, :32] = total.astype(BF16)
    sums = [got_ref[y, 16:].astype(F32).reshape(16, 8, 128) for y in range(4)]
    out_ref[:, 32:] = jnp.concatenate(sums, axis=1).astype(BF16)


def last_kernel(got_ref, own_ref, dk_ref, dv_ref, total_ref):
    total_ref[...] = got_ref[:, :32].astype(F32).sum(axis=0)
    sums = got_ref[:, 32:].reshape(512, 128)
    row = iota((256, 128), 0)
    first = (row & 31) * 16 + (row >> 5) - iota((256, 128), 1)
    for n, ref in enumerate((dk_ref, dv_ref)):
        perm = jnp.concatenate([one_hot(first == m * 128 - n * 8) for m in range(4)], axis=1)
        ref[...] = (dot(perm, sums) + own_ref[n].astype(F32)).astype(BF16)


VM = pl.BlockSpec(memory_space=pltpu.VMEM)
SM = pl.BlockSpec(memory_space=pltpu.SMEM)


def call(kernel, out, specs, *args, inputs=True, hbm=(), limit=0):
    if inputs:
        args = [pltpu.with_memory_space_constraint(a, pltpu.VMEM) if s is VM else a for a, s in zip(args, specs)]
    return pl.pallas_call(
        kernel,
        out_shape=[o if n in hbm else pltpu.VMEM(o.shape, o.dtype) for n, o in enumerate(out)],
        in_specs=specs,
        out_specs=[VM] * len(out),
        compiler_params=pltpu.CompilerParams(vmem_limit_bytes=limit << 20 if limit else None),
    )(*args)


def shape(*dims, dtype=BF16):
    return jax.ShapeDtypeStruct(dims, dtype)


def exchange(x, axis):
    return lax.all_to_all(x, axis, split_axis=0, concat_axis=0, tiled=True)


def shift(x, axis, by):
    size = lax.axis_size(axis)
    return lax.ppermute(x, axis, [(n, (n + by) % size) for n in range(size)])


def swapped(x):
    return lax.ppermute(x, "y", [(n, n ^ 1) for n in range(4)])


def body(queries, keys, values, log_sums, out_grad, chosen, normed):
    rows = queries.shape[0]
    base = ((lax.axis_index("z") * 4 + lax.axis_index("y")) & 7) * 16
    base = base.astype(jnp.int32).reshape(1)
    at_y, at_x, at_c = (lax.axis_index(axis).astype(jnp.int32).reshape(1) for axis in ("y", "x", "c"))
    (pieces,) = call(
        pack_kernel, [shape(1152, 128)], [SM, SM] + [VM] * 3, base, chosen, keys, values, normed, inputs=False
    )
    pieces = exchange(pieces.reshape(64, 9, 2, 128), KV)
    table, meta, half = (pieces[:, a:b].reshape(-1, 128) for a, b in ((0, 4), (4, 5), (5, 9)))
    picked, ids = call(select_kernel, [shape(1024, 128), shape(8, 128, dtype=F32)], [VM] * 2, table, meta)
    picked = exchange(picked.reshape(64, 16, 128), KV)
    (sent,) = call(sent_kernel, [shape(512, 128)], [SM] + [VM] * 3, at_y, ids, half, normed)
    other = swapped(sent)
    (features,) = call(turn_kernel, [shape(2, 128, 512)], [SM] + [VM] * 3, at_y, half, other, normed)
    parts = [features]
    for s in range(1, 4):
        parts.append(shift(features, "x", s))
    features = jnp.stack(parts)
    others = shift(features, "c", 1)
    query_grad, back, own = call(
        attend_kernel,
        [shape(rows, 128), shape(KB, 2, 16, 128), shape(2, rows, 128)],
        [SM] + [VM] * 6,
        chosen, queries, keys, values, out_grad, log_sums, picked.reshape(KB, 2, 16, 128),
        hbm=(0,),
    )
    back = exchange(back.reshape(64, 16, 128), KV)
    partner = lax.ppermute(own[1], "y", [(1, 0), (3, 2)])
    (sums,) = call(
        sum_kernel,
        [shape(4, 20, 32, 128)],
        [SM] * 3 + [VM] * 6,
        at_y, at_x, at_c, ids, back.reshape(1024, 128), own, partner, features, others,
        limit=24,
    )
    sums = exchange(sums, "y")
    (sums,) = call(middle_kernel, [shape(16, 64, 128)], [VM], sums)
    sums = exchange(sums, "z")
    key_grad, value_grad, weight_grad = call(
        last_kernel,
        [shape(rows, 128), shape(rows, 128), shape(32, 128, dtype=F32)],
        [VM] * 2,
        sums, own,
        hbm=(0, 1, 2),
    )
    return query_grad, key_grad, value_grad, weight_grad


def solution(mesh):
    fine = Mesh(mesh.devices.reshape(16, 4, 4, 2), ("z", "y", "x", "c"))
    both = P(KV, ("x", "c"))
    in_specs = (both, both, both, P(("x", "c"), KV), both, P(KV, None), both)
    return jax.shard_map(body, mesh=fine, in_specs=in_specs, out_specs=(both,) * 4, check_vma=False)
```

```python
import jax
import jax.numpy as jnp
from jax import lax
from jax.experimental import pallas as pl
from jax.experimental.pallas import tpu as pltpu
from jax.sharding import Mesh
from jax.sharding import PartitionSpec as P


KV = ("z", "y")
QB = 128
KB = 32
HD = 64
SEL = 8
F32 = jnp.float32
BF16 = jnp.bfloat16


def iota(shape, dim):
    return lax.broadcasted_iota(jnp.int32, shape, dim)


def dot(a, b, dims=((1,), (0,))):
    return lax.dot_general(a, b, (dims, ((), ())), preferred_element_type=F32)


def one_hot(hits):
    return jnp.where(hits, 1.0, 0.0).astype(BF16)


def pack_kernel(base_ref, chosen_ref, keys_ref, values_ref, normed_ref, out_ref):
    lane = iota((1, 128), 1)
    high = jnp.zeros((1, 128), F32)
    low = jnp.zeros((1, 128), F32)
    for g in range(2):
        for s in range(SEL):
            entry = chosen_ref[g, s] + 1
            here = lane == base_ref[0] + (g * SEL + s)
            high = jnp.where(here, (entry >> 3).astype(F32), high)
            low = jnp.where(here, (entry & 7).astype(F32), low)
    row = iota((64 * 18, 128), 0)
    piece = (row * 3641) >> 16
    kind = row - piece * 18
    source = jnp.where(kind < 8, kind * KB, 256 + (kind - 10) * KB) + (piece >> 1)
    source = jnp.where((kind == 8) | (kind == 9), -1, source) - iota((64 * 18, 128), 1)
    perm = jnp.concatenate([one_hot(source == n * 128) for n in range(4)], axis=1)
    pairs = jnp.concatenate([keys_ref[...], values_ref[...]], axis=1)
    both = dot(perm, jnp.concatenate([pairs, normed_ref[...]], axis=0))
    extra = jnp.where(kind == 8, high, 0.0) + jnp.where(kind == 9, low, 0.0)
    out_ref[...] = (jnp.where((piece & 1) == 0, both[:, :128], both[:, 128:]) + extra).astype(BF16)


def select_kernel(got_ref, meta_ref, out_ref, ids_ref):
    got = got_ref[...]
    meta = meta_ref[...]
    group, col = iota((8, 128), 0) * 16, iota((8, 128), 1)
    inside = (col >= group) & (col < group + 16)
    even = (col & 1) == 0
    ids = dot(one_hot(inside & even), meta) * 8.0 + dot(one_hot(inside & ~even), meta)
    ids_ref[...] = ids
    columns = ids.T
    number = (iota((128, 512), 1) + 1).astype(F32)
    hot = jnp.concatenate([one_hot(number == columns[:, j : j + 1]) for j in range(8)], axis=0)
    out_ref[...] = dot(hot, got).astype(BF16)


def sent_kernel(y_ref, ids_ref, mine_ref, normed_ref, out_ref):
    normed = normed_ref[...].astype(F32)
    normed = jnp.concatenate([normed[:, :128], normed[:, 128:]], axis=0)
    out_ref[...] = jnp.where((y_ref[0] & 1) == 1, normed, mine_ref[...].astype(F32)).astype(BF16)


def turn_kernel(y_ref, mine_ref, other_ref, normed_ref, out_ref):
    eye = one_hot(iota((512, 512), 0) == iota((512, 512), 1))
    other = other_ref[...].astype(F32)
    normed = normed_ref[...].astype(F32)
    for n in range(2):
        kept = other if n == 0 else mine_ref[...].astype(F32)
        owned = jnp.concatenate([normed[:, n * 128 : (n + 1) * 128], other[n * 256 : (n + 1) * 256]], axis=0)
        part = jnp.where((y_ref[0] & 1) == 1, kept, owned).astype(BF16)
        out_ref[n] = dot(part, eye, ((0,), (0,))).astype(BF16)


def attend_kernel(
    chosen_ref, queries_ref, keys_ref, values_ref, grad_ref, sums_ref, got_ref, back_ref, slopes_ref, low_ref
):
    mine = (iota((2 * QB, 128), 1) >= HD) == (iota((2 * QB, 128), 0) >= QB)
    causal = iota((QB, 2 * QB), 0) <= (iota((QB, 2 * QB), 1) & (QB - 1))
    sub = iota((SEL, 2 * QB), 0)
    for g in range(2):
        span = slice(g * QB, (g + 1) * QB)
        picked = []
        for n in range(2):
            picked.append(got_ref[:, n, g * SEL : (g + 1) * SEL, :].reshape(KB * SEL, 128))
        keys = jnp.concatenate([picked[0], keys_ref[span, :]], axis=0)
        values = jnp.concatenate([picked[1], values_ref[span, :]], axis=0)
        q = queries_ref[span, :].astype(F32) * (HD**-0.5)
        do = grad_ref[span, :].astype(F32)
        q = jnp.where(mine, jnp.concatenate([q, q], axis=0), 0.0).astype(BF16)
        do = jnp.where(mine, jnp.concatenate([do, do], axis=0), 0.0).astype(BF16)
        sums = jnp.concatenate([sums_ref[0:1, span], sums_ref[1:2, span]], axis=1)
        used = jnp.zeros((SEL, 2 * QB), jnp.int32)
        for s in range(SEL):
            used = jnp.where(sub == s, chosen_ref[g, s] + 1, used)
        used = (used > 0)[None]
        scores = dot(keys, q, ((1,), (1,)))
        dots = dot(values, do, ((1,), (1,)))
        raw = jnp.exp(scores - sums)
        picked = jnp.where(used, raw[: KB * SEL].reshape(KB, SEL, 2 * QB), 0.0).reshape(KB * SEL, 2 * QB)
        weights = jnp.concatenate([picked, jnp.where(causal, raw[KB * SEL :], 0.0)], axis=0)
        low = weights.astype(BF16)
        deltas = jnp.sum(low.astype(F32) * dots, axis=0, keepdims=True)
        slopes = (weights * (dots - deltas)).astype(BF16)
        slopes_ref[g] = slopes
        low_ref[g] = low
        dk = dot(slopes[: KB * SEL], q)
        dv = dot(low[: KB * SEL], do)
        back_ref[:, 0, g * SEL : (g + 1) * SEL, :] = dk.reshape(KB, SEL, 128).astype(BF16)
        back_ref[:, 1, g * SEL : (g + 1) * SEL, :] = dv.reshape(KB, SEL, 128).astype(BF16)


def rest_kernel(queries_ref, keys_ref, grad_ref, got_ref, slopes_ref, low_ref, dq_ref, own_ref):
    mine = (iota((2 * QB, 128), 1) >= HD) == (iota((2 * QB, 128), 0) >= QB)
    low_lanes = iota((QB, 128), 1) < HD
    for g in range(2):
        span = slice(g * QB, (g + 1) * QB)
        picked = got_ref[:, 0, g * SEL : (g + 1) * SEL, :].reshape(KB * SEL, 128)
        keys = jnp.concatenate([picked, keys_ref[span, :]], axis=0)
        q = queries_ref[span, :].astype(F32) * (HD**-0.5)
        do = grad_ref[span, :].astype(F32)
        q = jnp.where(mine, jnp.concatenate([q, q], axis=0), 0.0).astype(BF16)
        do = jnp.where(mine, jnp.concatenate([do, do], axis=0), 0.0).astype(BF16)
        slopes = slopes_ref[g]
        own_ref[0, span, :] = dot(slopes[KB * SEL :], q).astype(BF16)
        own_ref[1, span, :] = dot(low_ref[g, KB * SEL :, :], do).astype(BF16)
        dq = dot(slopes, keys, ((0,), (0,)))
        dq_ref[span, :] = (jnp.where(low_lanes, dq[:QB], dq[QB:]) * (HD**-0.5)).astype(BF16)


def sum_kernel(y_ref, x_ref, c_ref, ids_ref, got_ref, own_ref, partner_ref, mine_ref, other_ref, out_ref):
    number = (iota((512, 128), 0) + 1).astype(F32)
    hot = jnp.concatenate([one_hot(number == ids_ref[j : j + 1, :]) for j in range(8)], axis=1)
    sums = dot(hot, got_ref[...])
    owned = jnp.concatenate([own_ref[1], partner_ref[...]], axis=0).astype(F32)
    value = jnp.where((y_ref[0] & 1) == 1, sums, owned).astype(BF16)
    for c, features_ref in enumerate((mine_ref, other_ref)):
        part = dot(features_ref[...].reshape(1024, 512), value).astype(BF16).reshape(4, 2, 4, 32, 128)
        for s in range(4):
            t = ((x_ref[0] - s) & 3) * 2 + ((c_ref[0] + c) & 1)
            for zz in range(2):
                for y in range(4):
                    out_ref[y, t * 2 + zz] = part[s, zz, y]
    sums = sums.reshape(4, 4, 4, 8, 128)
    for y in range(4):
        out_ref[y, 16:] = sums[:, :, y].reshape(4, 32, 128).astype(BF16)


def middle_kernel(got_ref, out_ref):
    total = got_ref[0, :16].astype(F32)
    for y in range(1, 4):
        total = total + got_ref[y, :16].astype(F32)
    out_ref[:, :32] = total.astype(BF16)
    sums = [got_ref[y, 16:].astype(F32).reshape(16, 8, 128) for y in range(4)]
    out_ref[:, 32:] = jnp.concatenate(sums, axis=1).astype(BF16)


def last_kernel(got_ref, own_ref, dk_ref, dv_ref, total_ref):
    total_ref[...] = got_ref[:, :32].astype(F32).sum(axis=0)
    sums = got_ref[:, 32:].reshape(512, 128)
    row = iota((256, 128), 0)
    first = (row & 31) * 16 + (row >> 5) - iota((256, 128), 1)
    for n, ref in enumerate((dk_ref, dv_ref)):
        perm = jnp.concatenate([one_hot(first == m * 128 - n * 8) for m in range(4)], axis=1)
        ref[...] = (dot(perm, sums) + own_ref[n].astype(F32)).astype(BF16)


VM = pl.BlockSpec(memory_space=pltpu.VMEM)
SM = pl.BlockSpec(memory_space=pltpu.SMEM)


def call(kernel, out, specs, *args, inputs=True, hbm=(), limit=0):
    if inputs:
        args = [pltpu.with_memory_space_constraint(a, pltpu.VMEM) if s is VM else a for a, s in zip(args, specs)]
    return pl.pallas_call(
        kernel,
        out_shape=[o if n in hbm else pltpu.VMEM(o.shape, o.dtype) for n, o in enumerate(out)],
        in_specs=specs,
        out_specs=[VM] * len(out),
        compiler_params=pltpu.CompilerParams(vmem_limit_bytes=limit << 20 if limit else None),
    )(*args)


def shape(*dims, dtype=BF16):
    return jax.ShapeDtypeStruct(dims, dtype)


def exchange(x, axis):
    return lax.all_to_all(x, axis, split_axis=0, concat_axis=0, tiled=True)


def shift(x, axis, by):
    size = lax.axis_size(axis)
    return lax.ppermute(x, axis, [(n, (n + by) % size) for n in range(size)])


def swapped(x):
    return lax.ppermute(x, "y", [(n, n ^ 1) for n in range(4)])


def body(queries, keys, values, log_sums, out_grad, chosen, normed):
    rows = queries.shape[0]
    base = ((lax.axis_index("z") * 4 + lax.axis_index("y")) & 7) * 16
    base = base.astype(jnp.int32).reshape(1)
    at_y, at_x, at_c = (lax.axis_index(axis).astype(jnp.int32).reshape(1) for axis in ("y", "x", "c"))
    (pieces,) = call(
        pack_kernel, [shape(1152, 128)], [SM, SM] + [VM] * 3, base, chosen, keys, values, normed, inputs=False
    )
    pieces = exchange(pieces.reshape(64, 9, 2, 128), KV)
    table, meta, half = (pieces[:, a:b].reshape(-1, 128) for a, b in ((0, 4), (4, 5), (5, 9)))
    picked, ids = call(select_kernel, [shape(1024, 128), shape(8, 128, dtype=F32)], [VM] * 2, table, meta)
    picked = exchange(picked.reshape(64, 16, 128), KV)
    (sent,) = call(sent_kernel, [shape(512, 128)], [SM] + [VM] * 3, at_y, ids, half, normed)
    other = swapped(sent)
    (features,) = call(turn_kernel, [shape(2, 128, 512)], [SM] + [VM] * 3, at_y, half, other, normed)
    parts = [features]
    for s in range(1, 4):
        parts.append(shift(features, "x", s))
    features = jnp.stack(parts)
    others = shift(features, "c", 1)
    picked = picked.reshape(KB, 2, 16, 128)
    back, slopes, low = call(
        attend_kernel,
        [shape(KB, 2, 16, 128), shape(2, 384, 256), shape(2, 384, 256)],
        [SM] + [VM] * 6,
        chosen, queries, keys, values, out_grad, log_sums, picked,
    )
    query_grad, own = call(
        rest_kernel,
        [shape(rows, 128), shape(2, rows, 128)],
        [VM] * 6,
        queries, keys, out_grad, picked, slopes, low,
        hbm=(0,),
    )
    back = exchange(back.reshape(64, 16, 128), KV)
    partner = lax.ppermute(own[1], "y", [(1, 0), (3, 2)])
    (sums,) = call(
        sum_kernel,
        [shape(4, 20, 32, 128)],
        [SM] * 3 + [VM] * 6,
        at_y, at_x, at_c, ids, back.reshape(1024, 128), own, partner, features, others,
        limit=24,
    )
    sums = exchange(sums, "y")
    (sums,) = call(middle_kernel, [shape(16, 64, 128)], [VM], sums)
    sums = exchange(sums, "z")
    key_grad, value_grad, weight_grad = call(
        last_kernel,
        [shape(rows, 128), shape(rows, 128), shape(32, 128, dtype=F32)],
        [VM] * 2,
        sums, own,
        hbm=(0, 1, 2),
    )
    return query_grad, key_grad, value_grad, weight_grad


def solution(mesh):
    fine = Mesh(mesh.devices.reshape(16, 4, 4, 2), ("z", "y", "x", "c"))
    both = P(KV, ("x", "c"))
    in_specs = (both, both, both, P(("x", "c"), KV), both, P(KV, None), both)
    return jax.shard_map(body, mesh=fine, in_specs=in_specs, out_specs=(both,) * 4, check_vma=False)
```
